32 devices in a mesh: sp: 8 (over z, x), tp: 4 (over y, core).
Axes of the slice: x: 2, y: 2, z: 4, core: 2. Of those that a mesh axis runs over, the one named last changes fastest.
Arguments:
- inputs: bfloat16 [8192, 2048], P('sp'), may hold values from -6 to 6
- w_query: bfloat16 [2048, 2048], P(None, 'tp'), may hold values from -0.125 to 0.125
- w_key: bfloat16 [2048, 2048], P(None, 'tp'), may hold values from -0.125 to 0.125
- w_value: bfloat16 [2048, 2048], P(None, 'tp'), may hold values from -0.125 to 0.125
- rel_table: float32 [16, 257], P('tp'), may hold values from -4 to 254
- out_grad: bfloat16 [8192, 2048], P('sp', 'tp'), may hold values from -6 to 6
Outputs:
- query_grad: bfloat16 [8192, 2048], P('sp', 'tp')
- key_grad: bfloat16 [8192, 2048], P('sp', 'tp')
- value_grad: bfloat16 [8192, 2048], P('sp', 'tp')
- query_weight_grad: float32 [2048, 2048], P('sp', 'tp')
- key_weight_grad: float32 [2048, 2048], P('sp', 'tp')
- value_weight_grad: float32 [2048, 2048], P('sp', 'tp')
- table_grad: float32 [16, 257], P('tp')
The draws below stay inside these ranges and needn't reach their ends.
All inputs are finite; a program needn't handle non-finite values.
Results may differ from the reference program's by a relative error of at most 0.017.
The reference program's roundings to bfloat16 on the way count: a program that leaves them out, or rounds other values in their place, can miss the bound.
Values may be sent and summed in bfloat16 or wider, within the bound.
A program may use at most 128 MiB of HBM per device.

```python
import jax
import jax.numpy as jnp
from jax import lax

HEADS = 16
HDIM = 128
D = 2048
SEG = 64
PREV = 4
MAXREL = 128
TOKENS = 8192


def draw_rel_table(key, part):
    base_key = jax.random.fold_in(jax.random.fold_in(key, 7), 0)
    bias_table = jnp.clip(jax.random.normal(base_key, (HEADS, 2 * MAXREL + 1), jnp.float32), -4.0, 4.0)
    return bias_table


def strengthened(drawn, own_key, source, target, parts, factor):
    owner, partner = [(jnp.arange(drawn.shape[axis_at]) // (drawn.shape[axis_at] // parts)).reshape([-1 if axis == axis_at else 1 for axis in range(drawn.ndim)]) for axis_at in (source, target)]
    chosen = jax.random.permutation(own_key, parts)[partner]
    strong = (owner == chosen) | (owner == (partner + parts // 2) % parts)
    return jnp.where(strong, factor * drawn, drawn)


def block_scale(rng, extent, pieces, least, high):
    factor_of = 1.0
    for dim, parts in pieces:
        steps = jax.random.uniform(jax.random.fold_in(jax.random.fold_in(rng, 6), dim), (parts,), jnp.float32, least / len(pieces), high / len(pieces))
        factor_of = factor_of * jnp.repeat(jnp.exp(steps), extent[dim] // parts).reshape((-1,) + (1,) * (len(extent) - 1 - dim))
    return factor_of


def normal_values(key, shape, spread, most, cuts=(), kind=jnp.bfloat16):
    values = spread * jax.random.normal(key, shape, jnp.float32)
    if cuts:
        values = values * block_scale(key, shape, cuts, -0.22, 0.18)
    return jnp.clip(values, -most, most).astype(kind)


def bell_draw_with(rng, shape, spread, bound, shards, heavy, held_as=jnp.bfloat16):
    array = spread * jax.random.normal(rng, shape, jnp.float32)
    if shards:
        array = array * block_scale(rng, shape, shards, -0.22, 0.18)
    return jnp.clip(strengthened(array, jax.random.fold_in(rng, 3), *heavy), -bound, bound).astype(held_as)


def setup_inputs(seed: int = 0) -> dict:
    streams_of = jax.random.split(jax.random.key(seed), 7)
    return {
        "inputs": bell_draw_with(streams_of[0], (TOKENS, D), 1.0, 6.0, ((0, 8),), (0, 1, 8, 2.0)),
        "w_query": normal_values(streams_of[1], (D, D), D ** -0.5, 0.125, ((1, 4),)),
        "w_key": normal_values(streams_of[2], (D, D), D ** -0.5, 0.125, ((1, 4),)),
        "w_value": normal_values(streams_of[3], (D, D), D ** -0.5, 0.125, ((1, 4),)),
        "rel_table": draw_rel_table(jax.random.fold_in(streams_of[6], 71), 0),
        "out_grad": normal_values(streams_of[5], (TOKENS, D), 1.0, 6.0, ((0, 8), (1, 4))),
    }


def project(inputs, weight):
    return jnp.dot(inputs, weight, preferred_element_type=jnp.float32).astype(jnp.bfloat16)


def reference(inputs, w_query, w_key, w_value, rel_table, out_grad):
    reach = PREV * SEG
    band = reach + SEG
    score_scale = HDIM ** -0.5
    query = project(inputs, w_query).reshape(TOKENS, HEADS, HDIM)
    key_rows = project(inputs, w_key).reshape(TOKENS, HEADS, HDIM)
    value_rows = project(inputs, w_value).reshape(TOKENS, HEADS, HDIM)
    upstream = out_grad.reshape(TOKENS, HEADS, HDIM)
    key_pad = jnp.pad(key_rows, ((reach, 0), (0, 0), (0, 0)))
    value_pad = jnp.pad(value_rows, ((reach, 0), (0, 0), (0, 0)))
    row_index = jnp.arange(SEG, dtype=jnp.int32)[:, None]
    band_index = jnp.arange(band, dtype=jnp.int32)[None, :]
    buckets = jnp.clip(row_index + reach - band_index, -MAXREL, MAXREL) + MAXREL
    bias_pattern = rel_table[:, buckets].astype(jnp.float32)

    def one_segment(carry, segment):
        key_acc, value_acc, pattern = carry
        start = segment * SEG
        query_seg = lax.dynamic_slice_in_dim(query, start, SEG, 0).astype(jnp.float32)
        grad_seg = lax.dynamic_slice_in_dim(upstream, start, SEG, 0).astype(jnp.float32)
        key_band = lax.dynamic_slice_in_dim(key_pad, start, band, 0).astype(jnp.float32)
        value_band = lax.dynamic_slice_in_dim(value_pad, start, band, 0).astype(jnp.float32)
        visible = band_index[0] >= reach - start
        scores = jnp.einsum('qhd,khd->hqk', query_seg, key_band) * score_scale + bias_pattern
        scores = jnp.where(visible[None, None, :], scores, -jnp.inf)
        row_max = jnp.max(scores, axis=-1, keepdims=True)
        log_norm = row_max + jnp.log(jnp.sum(jnp.exp(scores - row_max), axis=-1, keepdims=True))
        probs_full = jnp.exp(scores - log_norm)
        probs_low = lax.optimization_barrier(probs_full.astype(jnp.bfloat16)).astype(jnp.float32)
        attn_out = jnp.einsum('hqk,khd->qhd', probs_low, value_band)
        attn_out = lax.optimization_barrier(attn_out.astype(jnp.bfloat16)).astype(jnp.float32)
        out_dot = jnp.sum(grad_seg * attn_out, axis=-1)
        value_part = jnp.einsum('hqk,qhd->khd', probs_low, grad_seg)
        prob_grad = jnp.einsum('qhd,khd->hqk', grad_seg, value_band)
        score_grad = probs_full * (prob_grad - jnp.transpose(out_dot)[:, :, None])
        score_low = lax.optimization_barrier(score_grad.astype(jnp.bfloat16)).astype(jnp.float32)
        query_part = score_scale * jnp.einsum('hqk,khd->qhd', score_low, key_band)
        key_part = score_scale * jnp.einsum('hqk,qhd->khd', score_low, query_seg)
        key_acc = lax.dynamic_update_slice_in_dim(
            key_acc, lax.dynamic_slice_in_dim(key_acc, start, band, 0) + key_part, start, 0)
        value_acc = lax.dynamic_update_slice_in_dim(
            value_acc, lax.dynamic_slice_in_dim(value_acc, start, band, 0) + value_part, start, 0)
        pattern = pattern + score_grad
        return (key_acc, value_acc, pattern), query_part.astype(jnp.bfloat16)

    initial = (jnp.zeros((TOKENS + reach, HEADS, HDIM), jnp.float32),
               jnp.zeros((TOKENS + reach, HEADS, HDIM), jnp.float32),
               jnp.zeros((HEADS, SEG, band), jnp.float32))
    (key_acc, value_acc, pattern), query_parts = lax.scan(
        one_segment, initial, jnp.arange(TOKENS // SEG, dtype=jnp.int32))
    query_grad = query_parts.reshape(TOKENS, D)
    key_grad = key_acc[reach:].reshape(TOKENS, D).astype(jnp.bfloat16)
    value_grad = value_acc[reach:].reshape(TOKENS, D).astype(jnp.bfloat16)
    one_hot = (buckets[:, :, None] == jnp.arange(2 * MAXREL + 1, dtype=jnp.int32)[None, None, :]).astype(jnp.float32)
    table_grad = jnp.einsum('hqk,qkr->hr', pattern, one_hot, precision=lax.Precision.HIGHEST)
    query_weight_grad = jnp.dot(inputs.T, query_grad, preferred_element_type=jnp.float32)
    key_weight_grad = jnp.dot(inputs.T, key_grad, preferred_element_type=jnp.float32)
    value_weight_grad = jnp.dot(inputs.T, value_grad, preferred_element_type=jnp.float32)
    return (query_grad, key_grad, value_grad, query_weight_grad, key_weight_grad, value_weight_grad, table_grad)
```

```python
import functools

import jax
import jax.numpy as jnp
from jax import lax
from jax.experimental import pallas as pl
from jax.experimental.pallas import tpu as pltpu
from jax.sharding import PartitionSpec as P


HDIM = 128
SEG = 64
PREV = 4
MAXREL = 128
REACH = PREV * SEG
TILE = 2 * SEG
BAND = REACH + TILE
WRAP = 4 * MAXREL
GROUPS = 2


def from_behind(block, axis, distance):
    devices = range(lax.axis_size(axis))
    route = [(i - distance, i) for i in devices if i - distance in devices]
    return lax.ppermute(block, axis, route)


def project(inputs, weight):
    return jnp.dot(inputs, weight, preferred_element_type=jnp.float32).astype(jnp.bfloat16)


def contract(a, b, dims):
    return lax.dot_general(a, b, (dims, ((), ())), preferred_element_type=jnp.float32)


def attention_kernel(
    first_ref, bias_ref, q_ref, k_ref, v_ref, g_ref, hk_ref, hv_ref,
    dq_ref, dk_ref, dv_ref, hdk_ref, hdv_ref, tk_ref, tv_ref, diag_ref,
    kx, vx, dk_acc, dv_acc, band_acc,
):
    rows = q_ref.shape[0]
    scale = HDIM ** (-0.5)
    kx[:REACH] = hk_ref[...]
    kx[REACH:] = k_ref[...]
    vx[:REACH] = hv_ref[...]
    vx[REACH:] = v_ref[...]
    dk_acc[...] = jnp.zeros_like(dk_acc)
    dv_acc[...] = jnp.zeros_like(dv_acc)
    band_acc[...] = jnp.zeros_like(band_acc)
    row = lax.broadcasted_iota(jnp.int32, (TILE, BAND), 0)
    col = lax.broadcasted_iota(jnp.int32, (TILE, BAND), 1)
    start = row // SEG * SEG
    seen = (col >= start) & (col < start + REACH + SEG)
    wide = jnp.broadcast_to(bias_ref[0], (TILE, WRAP))
    bias = pltpu.roll(wide, 0, 1, stride=1, stride_axis=0)[:, :BAND]
    bias = jnp.where(seen, bias, -jnp.inf)
    is_first = first_ref[0] == 0
    for blk in range(rows // TILE):
        lo = blk * TILE
        q = q_ref[lo : lo + TILE]
        g = g_ref[lo : lo + TILE]
        k = kx[lo : lo + BAND]
        v = vx[lo : lo + BAND]
        s = contract(q, k, ((1,), (1,))) * scale + bias
        if lo < REACH:
            s = jnp.where(is_first & (col < REACH - lo), -jnp.inf, s)
        m = jnp.max(s, axis=1, keepdims=True)
        e = jnp.exp(s - m)
        p = e * (1.0 / jnp.sum(e, axis=1, keepdims=True))
        p_low = p.astype(jnp.bfloat16)
        out = contract(p_low, v, ((1,), (0,))).astype(jnp.bfloat16)
        out_dot = jnp.sum(g.astype(jnp.float32) * out.astype(jnp.float32), axis=1, keepdims=True)
        dp = contract(g, v, ((1,), (1,)))
        ds = p * (dp - out_dot)
        ds_low = ds.astype(jnp.bfloat16)
        band_acc[:, :BAND] += ds
        dq_ref[lo : lo + TILE] = (contract(ds_low, k, ((1,), (0,))) * scale).astype(jnp.bfloat16)
        dk_acc[lo : lo + BAND] += contract(ds_low, q, ((0,), (0,)))
        dv_acc[lo : lo + BAND] += contract(p_low, g, ((0,), (0,)))
    dk_ref[...] = (dk_acc[REACH:] * scale).astype(jnp.bfloat16)
    dv_ref[...] = dv_acc[REACH:].astype(jnp.bfloat16)
    hdk_ref[...] = (dk_acc[:REACH] * scale).astype(jnp.bfloat16)
    hdv_ref[...] = dv_acc[:REACH].astype(jnp.bfloat16)
    tk_ref[...] = dk_acc[rows:] * scale
    tv_ref[...] = dv_acc[rows:]
    total = band_acc[...]
    half = TILE // 2
    while half >= 1:
        total = total[:half] + pltpu.roll(total[half:], WRAP - half, 1)
        half //= 2
    diag_ref[0] = total


def attention(first, bias_rows, query, keys, values, upstream, halo_k, halo_v, head0, heads):
    rows = query.shape[0]
    whole = pl.BlockSpec((rows, HDIM), lambda h: (0, h))
    shifted = pl.BlockSpec((rows, HDIM), lambda h: (0, head0 + h))
    edge = pl.BlockSpec((REACH, HDIM), lambda h: (0, h))
    line = pl.BlockSpec((1, 1, WRAP), lambda h: (head0 + h, 0, 0))
    width = heads * HDIM
    sds = jax.ShapeDtypeStruct
    flops = 12 * heads * rows * BAND * HDIM
    return pl.pallas_call(
        attention_kernel,
        grid=(heads,),
        in_specs=[pl.BlockSpec(memory_space=pltpu.SMEM), line, shifted, shifted, shifted, shifted,
                  pl.BlockSpec((REACH, HDIM), lambda h: (0, h)), pl.BlockSpec((REACH, HDIM), lambda h: (0, h))],
        out_specs=[whole, whole, whole, edge, edge, edge, edge,
                   pl.BlockSpec((1, 1, WRAP), lambda h: (h, 0, 0))],
        out_shape=[
            sds((rows, width), jnp.bfloat16), sds((rows, width), jnp.bfloat16), sds((rows, width), jnp.bfloat16),
            sds((REACH, width), jnp.bfloat16), sds((REACH, width), jnp.bfloat16),
            sds((REACH, width), jnp.float32), sds((REACH, width), jnp.float32),
            sds((heads, 1, WRAP), jnp.float32),
        ],
        scratch_shapes=[
            pltpu.VMEM((rows + REACH, HDIM), jnp.bfloat16), pltpu.VMEM((rows + REACH, HDIM), jnp.bfloat16),
            pltpu.VMEM((rows + REACH, HDIM), jnp.float32), pltpu.VMEM((rows + REACH, HDIM), jnp.float32),
            pltpu.VMEM((TILE, WRAP), jnp.float32),
        ],
        cost_estimate=pl.CostEstimate(flops=flops * 2, bytes_accessed=heads * rows * HDIM * 20, transcendentals=heads * rows * BAND),
    )(first, bias_rows, query, keys, values, upstream, halo_k, halo_v)


def swap(block, bit):
    size = lax.axis_size("sp")
    return lax.ppermute(block, "sp", [(i, i ^ (1 << bit)) for i in range(size)])


def side(pieces, lead, want):
    low = len(pieces)
    return [pieces[r] for r in range(low) if (r >> lead & 1) == want]


def product(lhs, grads):
    parts = [jnp.einsum("td,tc->dc", piece, grads, preferred_element_type=jnp.float32) for piece in lhs]
    return parts


def leading(pieces, grads, order):
    return jnp.concatenate([p.astype(jnp.bfloat16) for p in product(side(pieces, order[0], 1), grads)], axis=0)


def remainder(pieces, grads, order, came):
    total = jnp.concatenate(product(side(pieces, order[0], 0), grads), axis=0)
    return total + came.astype(jnp.float32)


def split(total, kept, bit):
    depth = total.shape[0] // len(kept)
    out = [i for i, r in enumerate(kept) if r >> bit & 1]
    stay = [i for i, r in enumerate(kept) if not r >> bit & 1]
    pick = lambda which: jnp.concatenate([total[i * depth : (i + 1) * depth] for i in which], axis=0)
    return pick(out).astype(jnp.bfloat16), pick(stay), [kept[i] for i in stay]


def staged_local(inputs, w_query, w_key, w_value, rel_table, out_grad):
    rows, model = inputs.shape
    head_count = w_query.shape[1] // HDIM
    size = lax.axis_size("sp")
    bits = size.bit_length() - 1
    me = lax.axis_index("sp")
    first = me.reshape(1)
    far = rel_table[:, 2 * MAXREL :]
    pad = jnp.broadcast_to(far, (head_count, MAXREL))
    bias_rows = jnp.concatenate([pad, rel_table[:, :0:-1], pad], axis=1)[:, None, :]
    keys = project(inputs, w_key)
    values = project(inputs, w_value)
    halo = from_behind(jnp.concatenate([keys[rows - REACH :], values[rows - REACH :]], axis=1), "sp", 1)
    query = project(inputs, w_query)
    width = head_count * HDIM
    heads = head_count // GROUPS
    span = heads * HDIM
    depth = model // size
    block = lambda r: lax.dynamic_slice(inputs, (0, (me ^ r) * depth), (rows, depth))
    low = min(size, 4)
    members = [[r for r in range(size) if r % low == p] for p in range(low)]
    pieces = [jnp.concatenate([block(r) for r in rs], axis=1) for rs in members]
    orders, ready = chunk_plan(bits)
    grads, chunks, flying, diags = [], [], [], []
    for group in range(GROUPS):
        at = group * span
        dq, dk, dv, hdk, hdv, tk, tv, diag = attention(
            first, bias_rows, query, keys, values, out_grad,
            halo[:, at : at + span], halo[:, width + at : width + at + span], group * heads, heads)
        back = jnp.concatenate([hdk, hdv], axis=1)
        sent = leading(pieces, dq, orders[3 * group])
        if group + 1 < GROUPS:
            back, sent, query = lax.optimization_barrier((back, sent, query))
        back = from_behind(back, "sp", -1).astype(jnp.float32)
        flying.append(swap(sent, orders[3 * group][0]))
        dk = lax.dynamic_update_slice(dk, (tk + back[:, :span]).astype(jnp.bfloat16), (rows - REACH, 0))
        dv = lax.dynamic_update_slice(dv, (tv + back[:, span:]).astype(jnp.bfloat16), (rows - REACH, 0))
        for i, grad in ((1, dk), (2, dv)):
            order = orders[3 * group + i]
            sent = leading(pieces, grad, order)
            flying.append(swap(sent, order[0]))
        grads.append((dq, dk, dv))
        chunks.extend((dq, dk, dv))
        diags.append(diag)
    count = len(chunks)
    kept = [[r for p in range(low) if not p >> order[0] & 1 for r in members[p]] for order in orders]
    held = [None] * count
    steps = sorted(((c, s) for c in range(count) for s in range(bits)), key=lambda cs: (ready[cs[0]] + 0.95 * cs[1], cs))
    last, done, hop = None, 0, 0
    diag = jnp.concatenate(diags, axis=0)[:, 0, :]
    table_came = swap(diag, 0)
    for c, stage in steps:
        came = flying[c]
        if last is not None:
            came, held[last] = lax.optimization_barrier((came, held[last]))
        if stage == 0:
            held[c] = remainder(pieces, chunks[c], orders[c], came)
        else:
            held[c] = held[c] + came.astype(jnp.float32)
        if stage + 1 < bits:
            bit = orders[c][stage + 1]
            out, held[c], kept[c] = split(held[c], kept[c], bit)
            flying[c] = swap(out, bit)
        last = c
        done += 1
        if hop < bits and done >= len(steps) * (hop + 1) // (bits + 1):
            came, held[c] = lax.optimization_barrier((table_came, held[c]))
            diag = diag + came
            hop += 1
            if hop < bits:
                table_came = swap(diag, hop)
    sums = [held[3 * group : 3 * group + 3] for group in range(GROUPS)]
    query_grad, key_grad, value_grad = [jnp.concatenate(parts, axis=1) for parts in zip(*grads)]
    wq, wk, wv = [jnp.concatenate(parts, axis=1) for parts in zip(*sums)]
    top = jnp.sum(diag[:, : MAXREL + 1], axis=1, keepdims=True) + jnp.sum(diag[:, 3 * MAXREL :], axis=1, keepdims=True)
    table_grad = jnp.concatenate(
        [jnp.zeros((head_count, 1), jnp.float32), diag[:, MAXREL + 1 : 3 * MAXREL][:, ::-1], top], axis=1)
    return query_grad, key_grad, value_grad, wq, wk, wv, table_grad


def fused_kernel(
    ways, bias_ref, x_hbm, wq_hbm, wk_hbm, wv_hbm, g_hbm,
    dq_hbm, dk_hbm, dv_hbm, gq_hbm, gk_hbm, gv_hbm, diag_ref,
    xb, wb, gb, qb, kv, dqb, dkb, dvb, dk_acc, dv_acc, band_acc, grads_t,
    near_out, near_in, own, far_out, far_in, back_out, back_in, diag_mine, diag_in, final,
    load_sem, store_sem, halo_s, halo_r, back_s, back_r, near_s, near_r, far_s, far_r, diag_s, diag_r,
):
    across, along = ways
    size = across * along
    heads, rows, _ = qb.shape
    model = xb.shape[1]
    depth = model // size
    scale = HDIM ** (-0.5)
    me = lax.axis_index("sp")
    xi = lax.rem(me, across)
    zi = me // across

    tail = pl.ds(rows - REACH, REACH)
    head_rows = pl.ds(0, rows - REACH)
    loads = [
        pltpu.make_async_copy(x_hbm.at[tail], xb.at[tail], load_sem.at[0]),
        pltpu.make_async_copy(wk_hbm, wb.at[0], load_sem.at[1]),
        pltpu.make_async_copy(wv_hbm, wb.at[1], load_sem.at[2]),
        pltpu.make_async_copy(x_hbm.at[head_rows], xb.at[head_rows], load_sem.at[3]),
        pltpu.make_async_copy(wq_hbm, wb.at[2], load_sem.at[4]),
    ]
    for h in range(heads):
        loads.append(pltpu.make_async_copy(g_hbm.at[:, h * HDIM : (h + 1) * HDIM], gb.at[h], load_sem.at[5 + h]))
    for copy in loads:
        copy.start()

    barrier = pltpu.get_barrier_semaphore()
    for k in range(1, size):
        pl.semaphore_signal(barrier, 1, device_id={"sp": lax.rem(me + k, size)})

    def halo(h):
        return pltpu.make_async_remote_copy(
            kv.at[:, h, pl.ds(rows, REACH)], kv.at[:, h, pl.ds(0, REACH)],
            halo_s.at[h], halo_r.at[h], device_id={"sp": lax.rem(me + 1, size)})

    def back(h):
        return pltpu.make_async_remote_copy(
            back_out.at[h], back_in.at[h], back_s.at[h], back_r.at[h],
            device_id={"sp": lax.rem(me + size - 1, size)})

    def near(h, dx, z):
        return pltpu.make_async_remote_copy(
            near_out.at[h, dx - 1, z], near_in.at[h, dx - 1, z],
            near_s.at[h, dx - 1, z], near_r.at[h, dx - 1, z],
            device_id={"sp": zi * across + lax.rem(xi + dx, across)})

    def far(h, dz):
        return pltpu.make_async_remote_copy(
            far_out.at[h, dz - 1], far_in.at[h, dz - 1], far_s.at[h, dz - 1], far_r.at[h, dz - 1],
            device_id={"sp": lax.rem(zi + dz, along) * across + xi})

    def share(k):
        return pltpu.make_async_remote_copy(
            diag_mine, diag_in.at[k - 1], diag_s.at[k - 1], diag_r.at[k - 1],
            device_id={"sp": lax.rem(me + k, size)})

    def place(which, at, value):
        for h in range(heads):
            kv[which, h, at] = value[:, h * HDIM : (h + 1) * HDIM]

    def dot_rows(at, which):
        return jnp.dot(xb[at], wb[which], preferred_element_type=jnp.float32).astype(jnp.bfloat16)

    @pl.when(me == 0)
    def _():
        kv[:, :, :REACH] = jnp.zeros((2, heads, REACH, HDIM), jnp.bfloat16)

    @pl.when(me == size - 1)
    def _():
        back_in[...] = jnp.zeros_like(back_in)

    loads[0].wait()
    loads[1].wait()
    place(0, pl.ds(rows, REACH), dot_rows(tail, 0))
    loads[2].wait()
    place(1, pl.ds(rows, REACH), dot_rows(tail, 1))
    pl.semaphore_wait(barrier, size - 1)

    @pl.when(me < size - 1)
    def _():
        for h in range(heads):
            halo(h).start()

    loads[3].wait()
    loads[4].wait()

    def project_chunk(c, carry):
        lo = pl.multiple_of(c * REACH, REACH)
        at = pl.ds(lo, REACH)
        dest = pl.ds(pl.multiple_of(lo + REACH, REACH), REACH)
        place(0, dest, dot_rows(at, 0))
        place(1, dest, dot_rows(at, 1))
        q = dot_rows(at, 2)
        for h in range(heads):
            qb[h, at] = q[:, h * HDIM : (h + 1) * HDIM]
        return carry

    lax.fori_loop(0, rows // REACH - 1, project_chunk, 0)
    q_tail = dot_rows(tail, 2)
    for h in range(heads):
        qb[h, tail] = q_tail[:, h * HDIM : (h + 1) * HDIM]
    for h in range(heads):
        loads[5 + h].wait()

    row = lax.broadcasted_iota(jnp.int32, (TILE, BAND), 0)
    col = lax.broadcasted_iota(jnp.int32, (TILE, BAND), 1)
    start = row // SEG * SEG
    seen = (col >= start) & (col < start + REACH + SEG)
    is_first = me == 0

    def attend(h):
        dk_acc[...] = jnp.zeros_like(dk_acc)
        dv_acc[...] = jnp.zeros_like(dv_acc)
        band_acc[...] = jnp.zeros_like(band_acc)
        wide = jnp.broadcast_to(bias_ref[h], (TILE, WRAP))
        bias = pltpu.roll(wide, 0, 1, stride=1, stride_axis=0)[:, :BAND]
        bias = jnp.where(seen, bias, -jnp.inf)

        @pl.when(me > 0)
        def _():
            halo(h).wait_recv()

        for blk in range(rows // TILE):
            lo = blk * TILE
            q = qb[h, lo : lo + TILE]
            g = gb[h, lo : lo + TILE]
            k = kv[0, h, lo : lo + BAND]
            v = kv[1, h, lo : lo + BAND]
            s = contract(q, k, ((1,), (1,))) * scale + bias
            if lo < REACH:
                s = jnp.where(is_first & (col < REACH - lo), -jnp.inf, s)
            m = jnp.max(s, axis=1, keepdims=True)
            e = jnp.exp(s - m)
            p = e * (1.0 / jnp.sum(e, axis=1, keepdims=True))
            p_low = p.astype(jnp.bfloat16)
            out = contract(p_low, v, ((1,), (0,))).astype(jnp.bfloat16)
            out_dot = jnp.sum(g.astype(jnp.float32) * out.astype(jnp.float32), axis=1, keepdims=True)
            dp = contract(g, v, ((1,), (1,)))
            ds = p * (dp - out_dot)
            ds_low = ds.astype(jnp.bfloat16)
            band_acc[:, :BAND] += ds
            dq = (contract(ds_low, k, ((1,), (0,))) * scale).astype(jnp.bfloat16)
            dqb[h, lo : lo + TILE] = dq
            grads_t[:HDIM, lo : lo + TILE] = dq.T
            dk_acc[lo : lo + BAND] += contract(ds_low, q, ((0,), (0,)))
            dv_acc[lo : lo + BAND] += contract(p_low, g, ((0,), (0,)))
            if lo + TILE == REACH:
                back_out[h, 0] = (dk_acc[:REACH] * scale).astype(jnp.bfloat16)
                back_out[h, 1] = dv_acc[:REACH].astype(jnp.bfloat16)

                @pl.when(me > 0)
                def _():
                    back(h).start()

        total = band_acc[...]
        half = TILE // 2
        while half >= 1:
            total = total[:half] + pltpu.roll(total[half:], WRAP - half, 1)
            half //= 2
        diag_mine[h] = total

        @pl.when(me < size - 1)
        def _():
            back(h).wait_recv()

        dk_acc[rows:] += back_in[h, 0].astype(jnp.float32) * (1.0 / scale)
        dv_acc[rows:] += back_in[h, 1].astype(jnp.float32)
        for lo in range(0, rows, REACH):
            dk = (dk_acc[REACH + lo : 2 * REACH + lo] * scale).astype(jnp.bfloat16)
            dv = dv_acc[REACH + lo : 2 * REACH + lo].astype(jnp.bfloat16)
            dkb[h, lo : lo + REACH] = dk
            dvb[h, lo : lo + REACH] = dv
            grads_t[HDIM : 2 * HDIM, lo : lo + REACH] = dk.T
            grads_t[2 * HDIM :, lo : lo + REACH] = dv.T
        for copy in stores(h):
            copy.start()

    def stores(h):
        cols = pl.ds(pl.multiple_of(h * HDIM, HDIM), HDIM)
        return [
            pltpu.make_async_copy(buf.at[h], out.at[:, cols], store_sem.at[i, h])
            for i, (buf, out) in enumerate(((dqb, dq_hbm), (dkb, dk_hbm), (dvb, dv_hbm)))
        ]

    def block_product(x, z):
        cols = pl.ds(pl.multiple_of((z * across + x) * depth, depth), depth)
        return jnp.dot(grads_t[...], xb[:, cols], preferred_element_type=jnp.float32)

    def multiply(h):
        def other(j, carry):
            z = lax.rem(zi + 1 + j, along)
            for dx in range(1, across):
                near_out[h, dx - 1, z] = block_product(lax.rem(xi + dx, across), z).astype(jnp.bfloat16)
                near(h, dx, z).start()
            return carry

        def mine(z, carry):
            own[h, z] = block_product(xi, z)
            return carry

        lax.fori_loop(0, along, other, 0)
        lax.fori_loop(0, along, mine, 0)

    def collect(h, z):
        total = own[h, z]
        for dx in range(1, across):
            near(h, dx, z).wait_recv()
            total = total + near_in[h, dx - 1, z].astype(jnp.float32)
        return total

    def forward(h):
        def one(dz, carry):
            z = lax.rem(zi + dz, along)
            far_out[h, dz - 1] = collect(h, z).astype(jnp.bfloat16)
            far(h, dz).start()
            return carry

        lax.fori_loop(1, along, one, 0)
        own[h, zi] = collect(h, zi)

    def finish(h):
        total = own[h, zi]
        for dz in range(1, along):
            far(h, dz).wait_recv()
            total = total + far_in[h, dz - 1].astype(jnp.float32)
        cols = pl.ds(pl.multiple_of(h * HDIM, HDIM), HDIM)
        for i in range(3):
            final[i, :, cols] = total[i * HDIM : (i + 1) * HDIM].T

    def one_head(h, carry):
        attend(h)
        multiply(h)

        @pl.when(h > 0)
        def _():
            forward(h - 1)

        return carry

    lax.fori_loop(0, heads, one_head, 0)
    for k in range(1, size):
        share(k).start()
    for h in range(heads - 2):
        finish(h)
    forward(heads - 1)
    for h in range(max(heads - 2, 0), heads):
        finish(h)
    results = [
        pltpu.make_async_copy(final.at[i], out, load_sem.at[i]) for i, out in enumerate((gq_hbm, gk_hbm, gv_hbm))
    ]
    for copy in results:
        copy.start()
    total = diag_mine[...]
    for k in range(1, size):
        share(k).wait_recv()
        total = total + diag_in[k - 1]
    diag_ref[...] = total
    for k in range(1, size):
        share(k).wait_send()
    for copy in results:
        copy.wait()

    @pl.when(me < size - 1)
    def _():
        for h in range(heads):
            halo(h).wait_send()

    @pl.when(me > 0)
    def _():
        for h in range(heads):
            back(h).wait_send()

    def drain(h, carry):
        for copy in stores(h):
            copy.wait()
        for dz in range(1, along):
            far(h, dz).wait_send()
        for dx in range(1, across):
            for z in range(along):
                near(h, dx, z).wait_send()
        return carry

    lax.fori_loop(0, heads, drain, 0)


def fused_local(inputs, w_query, w_key, w_value, rel_table, out_grad):
    rows, model = inputs.shape
    width = w_query.shape[1]
    heads = width // HDIM
    size = lax.axis_size("sp")
    across, along = grid_of(size)
    depth = model // size
    far = rel_table[:, 2 * MAXREL :]
    pad = jnp.broadcast_to(far, (heads, MAXREL))
    bias_rows = jnp.concatenate([pad, rel_table[:, :0:-1], pad], axis=1)[:, None, :]
    sds = jax.ShapeDtypeStruct
    bf16, f32 = jnp.bfloat16, jnp.float32
    any_space = pl.BlockSpec(memory_space=pl.ANY)
    vmem = pl.BlockSpec(memory_space=pltpu.VMEM)
    dma = pltpu.SemaphoreType.DMA
    dq, dk, dv, gq, gk, gv, diag = pl.pallas_call(
        functools.partial(fused_kernel, (across, along)),
        in_specs=[vmem] + [any_space] * 5,
        out_specs=[any_space] * 6 + [vmem],
        out_shape=[sds((rows, width), bf16)] * 3 + [sds((depth, width), f32)] * 3 + [sds((heads, 1, WRAP), f32)],
        scratch_shapes=[
            pltpu.VMEM((rows, model), bf16),
            pltpu.VMEM((3, model, width), bf16),
            pltpu.VMEM((heads, rows, HDIM), bf16),
            pltpu.VMEM((heads, rows, HDIM), bf16),
            pltpu.VMEM((2, heads, rows + REACH, HDIM), bf16),
            pltpu.VMEM((heads, rows, HDIM), bf16),
            pltpu.VMEM((heads, rows, HDIM), bf16),
            pltpu.VMEM((heads, rows, HDIM), bf16),
            pltpu.VMEM((rows + REACH, HDIM), f32),
            pltpu.VMEM((rows + REACH, HDIM), f32),
            pltpu.VMEM((TILE, WRAP), f32),
            pltpu.VMEM((3 * HDIM, rows), bf16),
            pltpu.VMEM((heads, across - 1, along, 3 * HDIM, depth), bf16),
            pltpu.VMEM((heads, across - 1, along, 3 * HDIM, depth), bf16),
            pltpu.VMEM((heads, along, 3 * HDIM, depth), f32),
            pltpu.VMEM((heads, along - 1, 3 * HDIM, depth), bf16),
            pltpu.VMEM((heads, along - 1, 3 * HDIM, depth), bf16),
            pltpu.VMEM((heads, 2, REACH, HDIM), bf16),
            pltpu.VMEM((heads, 2, REACH, HDIM), bf16),
            pltpu.VMEM((heads, 1, WRAP), f32),
            pltpu.VMEM((size - 1, heads, 1, WRAP), f32),
            pltpu.VMEM((3, depth, width), f32),
            dma((5 + heads,)), dma((3, heads)),
            dma((heads,)), dma((heads,)), dma((heads,)), dma((heads,)),
            dma((heads, across - 1, along)), dma((heads, across - 1, along)),
            dma((heads, along - 1)), dma((heads, along - 1)),
            dma((size - 1,)), dma((size - 1,)),
        ],
        compiler_params=pltpu.CompilerParams(collective_id=0, has_side_effects=True, vmem_limit_bytes=60 * 2**20),
    )(bias_rows, inputs, w_query, w_key, w_value, out_grad)
    diag = diag[:, 0, :]
    top = jnp.sum(diag[:, : MAXREL + 1], axis=1, keepdims=True) + jnp.sum(diag[:, 3 * MAXREL :], axis=1, keepdims=True)
    table_grad = jnp.concatenate(
        [jnp.zeros((heads, 1), f32), diag[:, MAXREL + 1 : 3 * MAXREL][:, ::-1], top], axis=1)
    return dq, dk, dv, gq, gk, gv, table_grad


def grid_of(size):
    across = 1 << ((size.bit_length() - 1) // 2)
    return across, size // across


def fits(size, rows, model, width):
    across, _ = grid_of(size)
    depth = model // size
    held = 2 * (rows * model + 3 * model * width + 7 * rows * width + 3 * model * width * 2) + 6 * model * width * 2
    return across > 1 and depth % HDIM == 0 and rows % REACH == 0 and rows > REACH and held < 56 * 2**20


def local(*args):
    inputs, w_query = args[:2]
    if fits(lax.axis_size("sp"), *inputs.shape, w_query.shape[1]):
        return fused_local(*args)
    return staged_local(*args)


def chunk_plan(bits):
    plain = list(range(bits))
    turned = [1, 0] + plain[2:] if bits > 1 else plain
    count = 3 * GROUPS
    orders = [plain] * (count - 2) + [turned] * 2
    ready = [1.0, 3.0, 4.0, 2.0, 3.9, 4.1]
    return orders, ready


def solution(mesh):
    placed = (
        P("sp", None),
        P(None, "tp"),
        P(None, "tp"),
        P(None, "tp"),
        P("tp", None),
        P("sp", "tp"),
    )
    return jax.shard_map(
        local,
        mesh=mesh,
        in_specs=placed,
        out_specs=(
            P("sp", "tp"),
            P("sp", "tp"),
            P("sp", "tp"),
            P("sp", "tp"),
            P("sp", "tp"),
            P("sp", "tp"),
            P("tp", None),
        ),
        check_vma=False,
    )
```

```python
import functools

import jax
import jax.numpy as jnp
from jax import lax
from jax.experimental import pallas as pl
from jax.experimental.pallas import tpu as pltpu
from jax.sharding import PartitionSpec as P


HDIM = 128
SEG = 64
PREV = 4
MAXREL = 128
REACH = PREV * SEG
TILE = 2 * SEG
BAND = REACH + TILE
WRAP = 4 * MAXREL
GROUPS = 2


def from_behind(block, axis, distance):
    devices = range(lax.axis_size(axis))
    route = [(i - distance, i) for i in devices if i - distance in devices]
    return lax.ppermute(block, axis, route)


def project(inputs, weight):
    return jnp.dot(inputs, weight, preferred_element_type=jnp.float32).astype(jnp.bfloat16)


def contract(a, b, dims):
    return lax.dot_general(a, b, (dims, ((), ())), preferred_element_type=jnp.float32)


def attention_kernel(
    first_ref, bias_ref, q_ref, k_ref, v_ref, g_ref, hk_ref, hv_ref,
    dq_ref, dk_ref, dv_ref, hdk_ref, hdv_ref, tk_ref, tv_ref, diag_ref,
    kx, vx, dk_acc, dv_acc, band_acc,
):
    rows = q_ref.shape[0]
    scale = HDIM ** (-0.5)
    kx[:REACH] = hk_ref[...]
    kx[REACH:] = k_ref[...]
    vx[:REACH] = hv_ref[...]
    vx[REACH:] = v_ref[...]
    dk_acc[...] = jnp.zeros_like(dk_acc)
    dv_acc[...] = jnp.zeros_like(dv_acc)
    band_acc[...] = jnp.zeros_like(band_acc)
    row = lax.broadcasted_iota(jnp.int32, (TILE, BAND), 0)
    col = lax.broadcasted_iota(jnp.int32, (TILE, BAND), 1)
    start = row // SEG * SEG
    seen = (col >= start) & (col < start + REACH + SEG)
    wide = jnp.broadcast_to(bias_ref[0], (TILE, WRAP))
    bias = pltpu.roll(wide, 0, 1, stride=1, stride_axis=0)[:, :BAND]
    bias = jnp.where(seen, bias, -jnp.inf)
    is_first = first_ref[0] == 0
    for blk in range(rows // TILE):
        lo = blk * TILE
        q = q_ref[lo : lo + TILE]
        g = g_ref[lo : lo + TILE]
        k = kx[lo : lo + BAND]
        v = vx[lo : lo + BAND]
        s = contract(q, k, ((1,), (1,))) * scale + bias
        if lo < REACH:
            s = jnp.where(is_first & (col < REACH - lo), -jnp.inf, s)
        m = jnp.max(s, axis=1, keepdims=True)
        e = jnp.exp(s - m)
        p = e * (1.0 / jnp.sum(e, axis=1, keepdims=True))
        p_low = p.astype(jnp.bfloat16)
        out = contract(p_low, v, ((1,), (0,))).astype(jnp.bfloat16)
        out_dot = jnp.sum(g.astype(jnp.float32) * out.astype(jnp.float32), axis=1, keepdims=True)
        dp = contract(g, v, ((1,), (1,)))
        ds = p * (dp - out_dot)
        ds_low = ds.astype(jnp.bfloat16)
        band_acc[:, :BAND] += ds
        dq_ref[lo : lo + TILE] = (contract(ds_low, k, ((1,), (0,))) * scale).astype(jnp.bfloat16)
        dk_acc[lo : lo + BAND] += contract(ds_low, q, ((0,), (0,)))
        dv_acc[lo : lo + BAND] += contract(p_low, g, ((0,), (0,)))
    dk_ref[...] = (dk_acc[REACH:] * scale).astype(jnp.bfloat16)
    dv_ref[...] = dv_acc[REACH:].astype(jnp.bfloat16)
    hdk_ref[...] = (dk_acc[:REACH] * scale).astype(jnp.bfloat16)
    hdv_ref[...] = dv_acc[:REACH].astype(jnp.bfloat16)
    tk_ref[...] = dk_acc[rows:] * scale
    tv_ref[...] = dv_acc[rows:]
    total = band_acc[...]
    half = TILE // 2
    while half >= 1:
        total = total[:half] + pltpu.roll(total[half:], WRAP - half, 1)
        half //= 2
    diag_ref[0] = total


def attention(first, bias_rows, query, keys, values, upstream, halo_k, halo_v, head0, heads):
    rows = query.shape[0]
    whole = pl.BlockSpec((rows, HDIM), lambda h: (0, h))
    shifted = pl.BlockSpec((rows, HDIM), lambda h: (0, head0 + h))
    edge = pl.BlockSpec((REACH, HDIM), lambda h: (0, h))
    line = pl.BlockSpec((1, 1, WRAP), lambda h: (head0 + h, 0, 0))
    width = heads * HDIM
    sds = jax.ShapeDtypeStruct
    flops = 12 * heads * rows * BAND * HDIM
    return pl.pallas_call(
        attention_kernel,
        grid=(heads,),
        in_specs=[pl.BlockSpec(memory_space=pltpu.SMEM), line, shifted, shifted, shifted, shifted,
                  pl.BlockSpec((REACH, HDIM), lambda h: (0, h)), pl.BlockSpec((REACH, HDIM), lambda h: (0, h))],
        out_specs=[whole, whole, whole, edge, edge, edge, edge,
                   pl.BlockSpec((1, 1, WRAP), lambda h: (h, 0, 0))],
        out_shape=[
            sds((rows, width), jnp.bfloat16), sds((rows, width), jnp.bfloat16), sds((rows, width), jnp.bfloat16),
            sds((REACH, width), jnp.bfloat16), sds((REACH, width), jnp.bfloat16),
            sds((REACH, width), jnp.float32), sds((REACH, width), jnp.float32),
            sds((heads, 1, WRAP), jnp.float32),
        ],
        scratch_shapes=[
            pltpu.VMEM((rows + REACH, HDIM), jnp.bfloat16), pltpu.VMEM((rows + REACH, HDIM), jnp.bfloat16),
            pltpu.VMEM((rows + REACH, HDIM), jnp.float32), pltpu.VMEM((rows + REACH, HDIM), jnp.float32),
            pltpu.VMEM((TILE, WRAP), jnp.float32),
        ],
        cost_estimate=pl.CostEstimate(flops=flops * 2, bytes_accessed=heads * rows * HDIM * 20, transcendentals=heads * rows * BAND),
    )(first, bias_rows, query, keys, values, upstream, halo_k, halo_v)


def swap(block, bit):
    size = lax.axis_size("sp")
    return lax.ppermute(block, "sp", [(i, i ^ (1 << bit)) for i in range(size)])


def side(pieces, lead, want):
    low = len(pieces)
    return [pieces[r] for r in range(low) if (r >> lead & 1) == want]


def product(lhs, grads):
    parts = [jnp.einsum("td,tc->dc", piece, grads, preferred_element_type=jnp.float32) for piece in lhs]
    return parts


def leading(pieces, grads, order):
    return jnp.concatenate([p.astype(jnp.bfloat16) for p in product(side(pieces, order[0], 1), grads)], axis=0)


def remainder(pieces, grads, order, came):
    total = jnp.concatenate(product(side(pieces, order[0], 0), grads), axis=0)
    return total + came.astype(jnp.float32)


def split(total, kept, bit):
    depth = total.shape[0] // len(kept)
    out = [i for i, r in enumerate(kept) if r >> bit & 1]
    stay = [i for i, r in enumerate(kept) if not r >> bit & 1]
    pick = lambda which: jnp.concatenate([total[i * depth : (i + 1) * depth] for i in which], axis=0)
    return pick(out).astype(jnp.bfloat16), pick(stay), [kept[i] for i in stay]


def staged_local(inputs, w_query, w_key, w_value, rel_table, out_grad):
    rows, model = inputs.shape
    head_count = w_query.shape[1] // HDIM
    size = lax.axis_size("sp")
    bits = size.bit_length() - 1
    me = lax.axis_index("sp")
    first = me.reshape(1)
    far = rel_table[:, 2 * MAXREL :]
    pad = jnp.broadcast_to(far, (head_count, MAXREL))
    bias_rows = jnp.concatenate([pad, rel_table[:, :0:-1], pad], axis=1)[:, None, :]
    keys = project(inputs, w_key)
    values = project(inputs, w_value)
    halo = from_behind(jnp.concatenate([keys[rows - REACH :], values[rows - REACH :]], axis=1), "sp", 1)
    query = project(inputs, w_query)
    width = head_count * HDIM
    heads = head_count // GROUPS
    span = heads * HDIM
    depth = model // size
    block = lambda r: lax.dynamic_slice(inputs, (0, (me ^ r) * depth), (rows, depth))
    low = min(size, 4)
    members = [[r for r in range(size) if r % low == p] for p in range(low)]
    pieces = [jnp.concatenate([block(r) for r in rs], axis=1) for rs in members]
    orders, ready = chunk_plan(bits)
    grads, chunks, flying, diags = [], [], [], []
    for group in range(GROUPS):
        at = group * span
        dq, dk, dv, hdk, hdv, tk, tv, diag = attention(
            first, bias_rows, query, keys, values, out_grad,
            halo[:, at : at + span], halo[:, width + at : width + at + span], group * heads, heads)
        back = jnp.concatenate([hdk, hdv], axis=1)
        sent = leading(pieces, dq, orders[3 * group])
        if group + 1 < GROUPS:
            back, sent, query = lax.optimization_barrier((back, sent, query))
        back = from_behind(back, "sp", -1).astype(jnp.float32)
        flying.append(swap(sent, orders[3 * group][0]))
        dk = lax.dynamic_update_slice(dk, (tk + back[:, :span]).astype(jnp.bfloat16), (rows - REACH, 0))
        dv = lax.dynamic_update_slice(dv, (tv + back[:, span:]).astype(jnp.bfloat16), (rows - REACH, 0))
        for i, grad in ((1, dk), (2, dv)):
            order = orders[3 * group + i]
            sent = leading(pieces, grad, order)
            flying.append(swap(sent, order[0]))
        grads.append((dq, dk, dv))
        chunks.extend((dq, dk, dv))
        diags.append(diag)
    count = len(chunks)
    kept = [[r for p in range(low) if not p >> order[0] & 1 for r in members[p]] for order in orders]
    held = [None] * count
    steps = sorted(((c, s) for c in range(count) for s in range(bits)), key=lambda cs: (ready[cs[0]] + 0.95 * cs[1], cs))
    last, done, hop = None, 0, 0
    diag = jnp.concatenate(diags, axis=0)[:, 0, :]
    table_came = swap(diag, 0)
    for c, stage in steps:
        came = flying[c]
        if last is not None:
            came, held[last] = lax.optimization_barrier((came, held[last]))
        if stage == 0:
            held[c] = remainder(pieces, chunks[c], orders[c], came)
        else:
            held[c] = held[c] + came.astype(jnp.float32)
        if stage + 1 < bits:
            bit = orders[c][stage + 1]
            out, held[c], kept[c] = split(held[c], kept[c], bit)
            flying[c] = swap(out, bit)
        last = c
        done += 1
        if hop < bits and done >= len(steps) * (hop + 1) // (bits + 1):
            came, held[c] = lax.optimization_barrier((table_came, held[c]))
            diag = diag + came
            hop += 1
            if hop < bits:
                table_came = swap(diag, hop)
    sums = [held[3 * group : 3 * group + 3] for group in range(GROUPS)]
    query_grad, key_grad, value_grad = [jnp.concatenate(parts, axis=1) for parts in zip(*grads)]
    wq, wk, wv = [jnp.concatenate(parts, axis=1) for parts in zip(*sums)]
    top = jnp.sum(diag[:, : MAXREL + 1], axis=1, keepdims=True) + jnp.sum(diag[:, 3 * MAXREL :], axis=1, keepdims=True)
    table_grad = jnp.concatenate(
        [jnp.zeros((head_count, 1), jnp.float32), diag[:, MAXREL + 1 : 3 * MAXREL][:, ::-1], top], axis=1)
    return query_grad, key_grad, value_grad, wq, wk, wv, table_grad


def fused_kernel(
    ways, bias_ref, x_hbm, wq_hbm, wk_hbm, wv_hbm, g_hbm,
    dq_hbm, dk_hbm, dv_hbm, gq_hbm, gk_hbm, gv_hbm, diag_ref,
    xb, wb, gb, qb, kv, dqb, dkb, dvb, dk_acc, dv_acc, band_acc, grads_t,
    near_out, near_in, own, far_out, far_in, relay_in, early_out, early_in, early_own, late_out, late_in,
    back_out, back_in, diag_mine, diag_in, final,
    load_sem, store_sem, halo_s, halo_r, back_s, back_r, near_s, near_r, far_s, far_r, relay_r,
    early_s, early_r, late_s, late_r, diag_s, diag_r,
):
    across, along, early = ways
    size = across * along
    heads, rows, _ = qb.shape
    model = xb.shape[1]
    depth = model // size
    scale = HDIM ** (-0.5)
    me = lax.axis_index("sp")
    xi = lax.rem(me, across)
    zi = me // across

    tail = pl.ds(rows - REACH, REACH)
    head_rows = pl.ds(0, rows - REACH)
    loads = [
        pltpu.make_async_copy(x_hbm.at[tail], xb.at[tail], load_sem.at[0]),
        pltpu.make_async_copy(wk_hbm, wb.at[0], load_sem.at[1]),
        pltpu.make_async_copy(wv_hbm, wb.at[1], load_sem.at[2]),
        pltpu.make_async_copy(x_hbm.at[head_rows], xb.at[head_rows], load_sem.at[3]),
        pltpu.make_async_copy(wq_hbm, wb.at[2], load_sem.at[4]),
    ]
    for h in range(heads):
        loads.append(pltpu.make_async_copy(g_hbm.at[:, h * HDIM : (h + 1) * HDIM], gb.at[h], load_sem.at[5 + h]))
    for copy in loads:
        copy.start()

    barrier = pltpu.get_barrier_semaphore()
    for k in range(1, size):
        pl.semaphore_signal(barrier, 1, device_id={"sp": lax.rem(me + k, size)})

    def halo(h):
        return pltpu.make_async_remote_copy(
            kv.at[:, h, pl.ds(rows, REACH)], kv.at[:, h, pl.ds(0, REACH)],
            halo_s.at[h], halo_r.at[h], device_id={"sp": lax.rem(me + 1, size)})

    def back(h):
        return pltpu.make_async_remote_copy(
            back_out.at[h], back_in.at[h], back_s.at[h], back_r.at[h],
            device_id={"sp": lax.rem(me + size - 1, size)})

    def used(h):
        return pl.ds(HDIM, 2 * HDIM) if h < early else pl.ds(0, 3 * HDIM)

    def at_z(z):
        return {"sp": z * across + xi}

    def at_x(x):
        return {"sp": zi * across + x}

    def near(h, dx, z):
        return pltpu.make_async_remote_copy(
            near_out.at[h, dx - 1, z, used(h)], near_in.at[h, dx - 1, z, used(h)],
            near_s.at[h, dx - 1, z], near_r.at[h, dx - 1, z], device_id=at_x(lax.rem(xi + dx, across)))

    def far(h, z):
        slot = lax.rem(z - zi + along, along) - 1
        return pltpu.make_async_remote_copy(
            far_out.at[h, z, used(h)], far_in.at[h, slot, used(h)], far_s.at[h, z], far_r.at[h, slot],
            device_id=at_z(z))

    def relay(h, z):
        step = jnp.where(z > zi, 1, -1)
        return pltpu.make_async_remote_copy(
            far_out.at[h, z, used(h)], relay_in.at[h, used(h)], far_s.at[h, z], relay_r.at[h],
            device_id=at_z(lax.rem(zi + step + along, along)))

    def early_copy(u, z):
        slot = lax.rem(z - zi + along, along) - 1
        return pltpu.make_async_remote_copy(
            early_out.at[u, z], early_in.at[u, slot], early_s.at[u, z], early_r.at[u, slot], device_id=at_z(z))

    def late_copy(u, dx):
        return pltpu.make_async_remote_copy(
            late_out.at[u, dx - 1], late_in.at[u, dx - 1], late_s.at[u, dx - 1], late_r.at[u, dx - 1],
            device_id=at_x(lax.rem(xi + dx, across)))

    relayed = along > 3

    def order(step):
        place = 0
        for z in range(along):
            others = sorted((t for t in range(along) if t != z), key=lambda t: hop_rank(z, t, along)) + [z]
            place = place + jnp.where(zi == z, others[step], 0)
        return place

    def share(k):
        return pltpu.make_async_remote_copy(
            diag_mine, diag_in.at[k - 1], diag_s.at[k - 1], diag_r.at[k - 1],
            device_id={"sp": lax.rem(me + k, size)})

    def place(which, at, value):
        for h in range(heads):
            kv[which, h, at] = value[:, h * HDIM : (h + 1) * HDIM]

    def dot_rows(at, which):
        return jnp.dot(xb[at], wb[which], preferred_element_type=jnp.float32).astype(jnp.bfloat16)

    @pl.when(me == 0)
    def _():
        kv[:, :, :REACH] = jnp.zeros((2, heads, REACH, HDIM), jnp.bfloat16)

    @pl.when(me == size - 1)
    def _():
        back_in[...] = jnp.zeros_like(back_in)

    loads[0].wait()
    loads[1].wait()
    place(0, pl.ds(rows, REACH), dot_rows(tail, 0))
    loads[2].wait()
    place(1, pl.ds(rows, REACH), dot_rows(tail, 1))
    pl.semaphore_wait(barrier, size - 1)

    @pl.when(me < size - 1)
    def _():
        for h in range(heads):
            halo(h).start()

    loads[3].wait()
    loads[4].wait()

    def project_chunk(c, carry):
        lo = pl.multiple_of(c * REACH, REACH)
        at = pl.ds(lo, REACH)
        dest = pl.ds(pl.multiple_of(lo + REACH, REACH), REACH)
        place(0, dest, dot_rows(at, 0))
        place(1, dest, dot_rows(at, 1))
        q = dot_rows(at, 2)
        for h in range(heads):
            qb[h, at] = q[:, h * HDIM : (h + 1) * HDIM]
        return carry

    lax.fori_loop(0, rows // REACH - 1, project_chunk, 0)
    q_tail = dot_rows(tail, 2)
    for h in range(heads):
        qb[h, tail] = q_tail[:, h * HDIM : (h + 1) * HDIM]
    for h in range(heads):
        loads[5 + h].wait()

    row = lax.broadcasted_iota(jnp.int32, (TILE, BAND), 0)
    col = lax.broadcasted_iota(jnp.int32, (TILE, BAND), 1)
    start = row // SEG * SEG
    seen = (col >= start) & (col < start + REACH + SEG)
    is_first = me == 0

    def block(h, blk, bias):
        lo = blk * TILE
        q = qb[h, lo : lo + TILE]
        g = gb[h, lo : lo + TILE]
        k = kv[0, h, lo : lo + BAND]
        v = kv[1, h, lo : lo + BAND]
        s = contract(q, k, ((1,), (1,))) * scale + bias
        if lo < REACH:
            s = jnp.where(is_first & (col < REACH - lo), -jnp.inf, s)
        m = jnp.max(s, axis=1, keepdims=True)
        e = jnp.exp(s - m)
        p = e * (1.0 / jnp.sum(e, axis=1, keepdims=True))
        p_low = p.astype(jnp.bfloat16)
        out = contract(p_low, v, ((1,), (0,))).astype(jnp.bfloat16)
        out_dot = jnp.sum(g.astype(jnp.float32) * out.astype(jnp.float32), axis=1, keepdims=True)
        dp = contract(g, v, ((1,), (1,)))
        ds = p * (dp - out_dot)
        ds_low = ds.astype(jnp.bfloat16)
        band_acc[h, :, :BAND] += ds
        dq = (contract(ds_low, k, ((1,), (0,))) * scale).astype(jnp.bfloat16)
        dqb[h, lo : lo + TILE] = dq
        grads_t[h, :HDIM, lo : lo + TILE] = dq.T
        dk_acc[h, lo : lo + BAND] += contract(ds_low, q, ((0,), (0,)))
        dv_acc[h, lo : lo + BAND] += contract(p_low, g, ((0,), (0,)))

    def bias_of(h):
        wide = jnp.broadcast_to(bias_ref[h], (TILE, WRAP))
        bias = pltpu.roll(wide, 0, 1, stride=1, stride_axis=0)[:, :BAND]
        return jnp.where(seen, bias, -jnp.inf)

    def attend_edge(h, carry):
        dk_acc[h] = jnp.zeros(dk_acc.shape[1:], jnp.float32)
        dv_acc[h] = jnp.zeros(dv_acc.shape[1:], jnp.float32)
        band_acc[h] = jnp.zeros(band_acc.shape[1:], jnp.float32)
        bias = bias_of(h)

        @pl.when(me > 0)
        def _():
            halo(h).wait_recv()

        for blk in range(REACH // TILE):
            block(h, blk, bias)
        back_out[h, 0] = (dk_acc[h, :REACH] * scale).astype(jnp.bfloat16)
        back_out[h, 1] = dv_acc[h, :REACH].astype(jnp.bfloat16)

        @pl.when(me > 0)
        def _():
            back(h).start()

        return carry

    def attend(h):
        bias = bias_of(h)
        for blk in range(REACH // TILE, rows // TILE):
            block(h, blk, bias)
        total = band_acc[h]
        half = TILE // 2
        while half >= 1:
            total = total[:half] + pltpu.roll(total[half:], WRAP - half, 1)
            half //= 2
        diag_mine[h] = total

        @pl.when(me < size - 1)
        def _():
            back(h).wait_recv()

        dk_acc[h, rows:] += back_in[h, 0].astype(jnp.float32) * (1.0 / scale)
        dv_acc[h, rows:] += back_in[h, 1].astype(jnp.float32)
        for lo in range(0, rows, REACH):
            dk = (dk_acc[h, REACH + lo : 2 * REACH + lo] * scale).astype(jnp.bfloat16)
            dv = dv_acc[h, REACH + lo : 2 * REACH + lo].astype(jnp.bfloat16)
            dkb[h, lo : lo + REACH] = dk
            dvb[h, lo : lo + REACH] = dv
            grads_t[h, HDIM : 2 * HDIM, lo : lo + REACH] = dk.T
            grads_t[h, 2 * HDIM :, lo : lo + REACH] = dv.T
        for copy in stores(h):
            copy.start()

    def stores(h):
        cols = pl.ds(pl.multiple_of(h * HDIM, HDIM), HDIM)
        return [
            pltpu.make_async_copy(buf.at[h], out.at[:, cols], store_sem.at[i, h])
            for i, (buf, out) in enumerate(((dqb, dq_hbm), (dkb, dk_hbm), (dvb, dv_hbm)))
        ]

    def columns(x, z):
        return pl.ds(pl.multiple_of((z * across + x) * depth, depth), depth)

    def product(h, part, cols):
        return jnp.dot(grads_t[h, part], xb[:, cols], preferred_element_type=jnp.float32)

    def multiply_early(h):
        part = pl.ds(0, HDIM)
        for step in range(along):
            z = order(step)
            cols = pl.ds(pl.multiple_of(z * across * depth, across * depth), across * depth)
            if step < along - 1:
                early_out[h, z] = product(h, part, cols).astype(jnp.bfloat16)
                early_copy(h, z).start()
            else:
                early_own[h] = product(h, part, cols)

    def multiply(h):
        for step in range(along):
            z = order(step)
            for dx in range(1, across):
                near_out[h, dx - 1, z, used(h)] = product(
                    h, used(h), columns(lax.rem(xi + dx, across), z)).astype(jnp.bfloat16)
                near(h, dx, z).start()

        def mine(z, carry):
            own[h, z, used(h)] = product(h, used(h), columns(xi, z))
            return carry

        lax.fori_loop(0, along, mine, 0)

    def collect(h, z):
        total = own[h, z, used(h)]
        for dx in range(1, across):
            near(h, dx, z).wait_recv()
            total = total + near_in[h, dx - 1, z, used(h)].astype(jnp.float32)
        return total

    def ends(z):
        return ((zi == 0) & (z == along - 1)) | ((zi == along - 1) & (z == 0))

    def joins(z):
        return ((zi == 1) & (z == along - 1)) | ((zi == along - 2) & (z == 0))

    def forward(h):
        for step in range(along - 1):
            z = order(step)
            total = collect(h, z)
            if not relayed:
                far_out[h, z, used(h)] = total.astype(jnp.bfloat16)
                far(h, z).start()
                continue

            @pl.when(joins(z))
            def _():
                relay(h, z).wait_recv()
                far_out[h, z, used(h)] = (total + relay_in[h, used(h)].astype(jnp.float32)).astype(jnp.bfloat16)

            @pl.when(jnp.logical_not(joins(z)))
            def _():
                far_out[h, z, used(h)] = total.astype(jnp.bfloat16)

            @pl.when(ends(z))
            def _():
                relay(h, z).start()

            @pl.when(jnp.logical_not(ends(z)))
            def _():
                far(h, z).start()

        own[h, zi, used(h)] = collect(h, zi)

    def turn(u):
        total = early_own[u]
        for dz in range(1, along):
            early_copy(u, lax.rem(zi + dz, along)).wait_recv()
            total = total + early_in[u, dz - 1].astype(jnp.float32)
        early_own[u] = total
        for dx in range(1, across):
            cols = pl.ds(pl.multiple_of(lax.rem(xi + dx, across) * depth, depth), depth)
            late_out[u, dx - 1] = early_own[u, :, cols].astype(jnp.bfloat16)
            late_copy(u, dx).start()

    def deliver(h, i, total):
        final[i, :, h * HDIM : (h + 1) * HDIM] = total.T

    def finish_early(u):
        total = early_own[u, :, pl.ds(pl.multiple_of(xi * depth, depth), depth)]
        for dx in range(1, across):
            late_copy(u, dx).wait_recv()
            total = total + late_in[u, dx - 1].astype(jnp.float32)
        deliver(u, 0, total)

    def arrives(dz):
        if not relayed:
            return None
        source = lax.rem(zi - dz + along, along)
        return jnp.logical_not(((source == 0) & (zi == along - 1)) | ((source == along - 1) & (zi == 0)))

    def finish(h):
        lead = 1 if h < early else 0
        for dz in range(1, along):
            def add():
                far(h, lax.rem(zi + dz, along)).wait_recv()
                own[h, zi, used(h)] += far_in[h, dz - 1, used(h)].astype(jnp.float32)

            if relayed:
                pl.when(arrives(dz))(add)
            else:
                add()
        for i in range(lead, 3):
            deliver(h, i, own[h, zi, i * HDIM : (i + 1) * HDIM])

    lax.fori_loop(0, heads, attend_edge, 0)
    for h in range(heads):
        attend(h)
        if h < early:
            multiply_early(h)
        multiply(h)
        if h > 0:
            forward(h - 1)
        if 2 <= h < early + 2:
            turn(h - 2)
    for k in range(1, size):
        share(k).start()
    for h in range(heads - 2):
        finish(h)
    for u in range(max(heads - 2, 0), early):
        turn(u)
    forward(heads - 1)
    for u in range(early):
        finish_early(u)
    for h in range(max(heads - 2, 0), heads):
        finish(h)
    results = [
        pltpu.make_async_copy(final.at[i], out, load_sem.at[i]) for i, out in enumerate((gq_hbm, gk_hbm, gv_hbm))
    ]
    for copy in results:
        copy.start()
    total = diag_mine[...]
    for k in range(1, size):
        share(k).wait_recv()
        total = total + diag_in[k - 1]
    diag_ref[...] = total
    for k in range(1, size):
        share(k).wait_send()
    for copy in results:
        copy.wait()

    @pl.when(me < size - 1)
    def _():
        for h in range(heads):
            halo(h).wait_send()

    @pl.when(me > 0)
    def _():
        for h in range(heads):
            back(h).wait_send()

    for h in range(heads):
        for copy in stores(h):
            copy.wait()
        for step in range(along - 1):
            far(h, order(step)).wait_send()
        for dx in range(1, across):
            for z in range(along):
                near(h, dx, z).wait_send()
    for u in range(early):
        for step in range(along - 1):
            early_copy(u, order(step)).wait_send()
        for dx in range(1, across):
            late_copy(u, dx).wait_send()


def hop_rank(here, there, along):
    far_end = abs(there - here) == along - 1
    joined = (here == 1 and there == along - 1) or (here == along - 2 and there == 0)
    return (joined, not far_end, -abs(there - here), there)


def fused_local(inputs, w_query, w_key, w_value, rel_table, out_grad):
    rows, model = inputs.shape
    width = w_query.shape[1]
    heads = width // HDIM
    size = lax.axis_size("sp")
    across, along = grid_of(size)
    early = heads // 2
    depth = model // size
    far = rel_table[:, 2 * MAXREL :]
    pad = jnp.broadcast_to(far, (heads, MAXREL))
    bias_rows = jnp.concatenate([pad, rel_table[:, :0:-1], pad], axis=1)[:, None, :]
    sds = jax.ShapeDtypeStruct
    bf16, f32 = jnp.bfloat16, jnp.float32
    any_space = pl.BlockSpec(memory_space=pl.ANY)
    vmem = pl.BlockSpec(memory_space=pltpu.VMEM)
    dma = pltpu.SemaphoreType.DMA
    dq, dk, dv, gq, gk, gv, diag = pl.pallas_call(
        functools.partial(fused_kernel, (across, along, early)),
        in_specs=[vmem] + [any_space] * 5,
        out_specs=[any_space] * 6 + [vmem],
        out_shape=[sds((rows, width), bf16)] * 3 + [sds((depth, width), f32)] * 3 + [sds((heads, 1, WRAP), f32)],
        scratch_shapes=[
            pltpu.VMEM((rows, model), bf16),
            pltpu.VMEM((3, model, width), bf16),
            pltpu.VMEM((heads, rows, HDIM), bf16),
            pltpu.VMEM((heads, rows, HDIM), bf16),
            pltpu.VMEM((2, heads, rows + REACH, HDIM), bf16),
            pltpu.VMEM((heads, rows, HDIM), bf16),
            pltpu.VMEM((heads, rows, HDIM), bf16),
            pltpu.VMEM((heads, rows, HDIM), bf16),
            pltpu.VMEM((heads, rows + REACH, HDIM), f32),
            pltpu.VMEM((heads, rows + REACH, HDIM), f32),
            pltpu.VMEM((heads, TILE, WRAP), f32),
            pltpu.VMEM((heads, 3 * HDIM, rows), bf16),
            pltpu.VMEM((heads, across - 1, along, 3 * HDIM, depth), bf16),
            pltpu.VMEM((heads, across - 1, along, 3 * HDIM, depth), bf16),
            pltpu.VMEM((heads, along, 3 * HDIM, depth), f32),
            pltpu.VMEM((heads, along, 3 * HDIM, depth), bf16),
            pltpu.VMEM((heads, along - 1, 3 * HDIM, depth), bf16),
            pltpu.VMEM((heads, 3 * HDIM, depth), bf16),
            pltpu.VMEM((early, along, HDIM, across * depth), bf16),
            pltpu.VMEM((early, along - 1, HDIM, across * depth), bf16),
            pltpu.VMEM((early, HDIM, across * depth), f32),
            pltpu.VMEM((early, across - 1, HDIM, depth), bf16),
            pltpu.VMEM((early, across - 1, HDIM, depth), bf16),
            pltpu.VMEM((heads, 2, REACH, HDIM), bf16),
            pltpu.VMEM((heads, 2, REACH, HDIM), bf16),
            pltpu.VMEM((heads, 1, WRAP), f32),
            pltpu.VMEM((size - 1, heads, 1, WRAP), f32),
            pltpu.VMEM((3, depth, width), f32),
            dma((5 + heads,)), dma((3, heads)),
            dma((heads,)), dma((heads,)), dma((heads,)), dma((heads,)),
            dma((heads, across - 1, along)), dma((heads, across - 1, along)),
            dma((heads, along)), dma((heads, along - 1)), dma((heads,)),
            dma((early, along)), dma((early, along - 1)), dma((early, across - 1)), dma((early, across - 1)),
            dma((size - 1,)), dma((size - 1,)),
        ],
        compiler_params=pltpu.CompilerParams(collective_id=0, has_side_effects=True, vmem_limit_bytes=60 * 2**20),
    )(bias_rows, inputs, w_query, w_key, w_value, out_grad)
    diag = diag[:, 0, :]
    top = jnp.sum(diag[:, : MAXREL + 1], axis=1, keepdims=True) + jnp.sum(diag[:, 3 * MAXREL :], axis=1, keepdims=True)
    table_grad = jnp.concatenate(
        [jnp.zeros((heads, 1), f32), diag[:, MAXREL + 1 : 3 * MAXREL][:, ::-1], top], axis=1)
    return dq, dk, dv, gq, gk, gv, table_grad


def grid_of(size):
    across = 1 << ((size.bit_length() - 1) // 2)
    return across, size // across


def fits(size, rows, model, width):
    across, _ = grid_of(size)
    depth = model // size
    held = 2 * (rows * model + 3 * model * width + 7 * rows * width + 3 * model * width * 2) + 6 * model * width * 2
    return across > 1 and depth % HDIM == 0 and rows % REACH == 0 and rows > REACH and held < 56 * 2**20


def local(*args):
    inputs, w_query = args[:2]
    if fits(lax.axis_size("sp"), *inputs.shape, w_query.shape[1]):
        return fused_local(*args)
    return staged_local(*args)


def chunk_plan(bits):
    plain = list(range(bits))
    turned = [1, 0] + plain[2:] if bits > 1 else plain
    count = 3 * GROUPS
    orders = [plain] * (count - 2) + [turned] * 2
    ready = [1.0, 3.0, 4.0, 2.0, 3.9, 4.1]
    return orders, ready


def solution(mesh):
    placed = (
        P("sp", None),
        P(None, "tp"),
        P(None, "tp"),
        P(None, "tp"),
        P("tp", None),
        P("sp", "tp"),
    )
    return jax.shard_map(
        local,
        mesh=mesh,
        in_specs=placed,
        out_specs=(
            P("sp", "tp"),
            P("sp", "tp"),
            P("sp", "tp"),
            P("sp", "tp"),
            P("sp", "tp"),
            P("sp", "tp"),
            P("tp", None),
        ),
        check_vma=False,
    )
```

```python
import functools

import jax
import jax.numpy as jnp
from jax import lax
from jax.experimental import pallas as pl
from jax.experimental.pallas import tpu as pltpu
from jax.sharding import PartitionSpec as P


HDIM = 128
SEG = 64
PREV = 4
MAXREL = 128
REACH = PREV * SEG
TILE = 2 * SEG
BAND = REACH + TILE
WRAP = 4 * MAXREL
GROUPS = 2


def from_behind(block, axis, distance):
    devices = range(lax.axis_size(axis))
    route = [(i - distance, i) for i in devices if i - distance in devices]
    return lax.ppermute(block, axis, route)


def project(inputs, weight):
    return jnp.dot(inputs, weight, preferred_element_type=jnp.float32).astype(jnp.bfloat16)


def contract(a, b, dims):
    return lax.dot_general(a, b, (dims, ((), ())), preferred_element_type=jnp.float32)


def attention_kernel(
    first_ref, bias_ref, q_ref, k_ref, v_ref, g_ref, hk_ref, hv_ref,
    dq_ref, dk_ref, dv_ref, hdk_ref, hdv_ref, tk_ref, tv_ref, diag_ref,
    kx, vx, dk_acc, dv_acc, band_acc,
):
    rows = q_ref.shape[0]
    scale = HDIM ** (-0.5)
    kx[:REACH] = hk_ref[...]
    kx[REACH:] = k_ref[...]
    vx[:REACH] = hv_ref[...]
    vx[REACH:] = v_ref[...]
    dk_acc[...] = jnp.zeros_like(dk_acc)
    dv_acc[...] = jnp.zeros_like(dv_acc)
    band_acc[...] = jnp.zeros_like(band_acc)
    row = lax.broadcasted_iota(jnp.int32, (TILE, BAND), 0)
    col = lax.broadcasted_iota(jnp.int32, (TILE, BAND), 1)
    start = row // SEG * SEG
    seen = (col >= start) & (col < start + REACH + SEG)
    wide = jnp.broadcast_to(bias_ref[0], (TILE, WRAP))
    bias = pltpu.roll(wide, 0, 1, stride=1, stride_axis=0)[:, :BAND]
    bias = jnp.where(seen, bias, -jnp.inf)
    is_first = first_ref[0] == 0
    for blk in range(rows // TILE):
        lo = blk * TILE
        q = q_ref[lo : lo + TILE]
        g = g_ref[lo : lo + TILE]
        k = kx[lo : lo + BAND]
        v = vx[lo : lo + BAND]
        s = contract(q, k, ((1,), (1,))) * scale + bias
        if lo < REACH:
            s = jnp.where(is_first & (col < REACH - lo), -jnp.inf, s)
        m = jnp.max(s, axis=1, keepdims=True)
        e = jnp.exp(s - m)
        p = e * (1.0 / jnp.sum(e, axis=1, keepdims=True))
        p_low = p.astype(jnp.bfloat16)
        out = contract(p_low, v, ((1,), (0,))).astype(jnp.bfloat16)
        out_dot = jnp.sum(g.astype(jnp.float32) * out.astype(jnp.float32), axis=1, keepdims=True)
        dp = contract(g, v, ((1,), (1,)))
        ds = p * (dp - out_dot)
        ds_low = ds.astype(jnp.bfloat16)
        band_acc[:, :BAND] += ds
        dq_ref[lo : lo + TILE] = (contract(ds_low, k, ((1,), (0,))) * scale).astype(jnp.bfloat16)
        dk_acc[lo : lo + BAND] += contract(ds_low, q, ((0,), (0,)))
        dv_acc[lo : lo + BAND] += contract(p_low, g, ((0,), (0,)))
    dk_ref[...] = (dk_acc[REACH:] * scale).astype(jnp.bfloat16)
    dv_ref[...] = dv_acc[REACH:].astype(jnp.bfloat16)
    hdk_ref[...] = (dk_acc[:REACH] * scale).astype(jnp.bfloat16)
    hdv_ref[...] = dv_acc[:REACH].astype(jnp.bfloat16)
    tk_ref[...] = dk_acc[rows:] * scale
    tv_ref[...] = dv_acc[rows:]
    total = band_acc[...]
    half = TILE // 2
    while half >= 1:
        total = total[:half] + pltpu.roll(total[half:], WRAP - half, 1)
        half //= 2
    diag_ref[0] = total


def attention(first, bias_rows, query, keys, values, upstream, halo_k, halo_v, head0, heads):
    rows = query.shape[0]
    whole = pl.BlockSpec((rows, HDIM), lambda h: (0, h))
    shifted = pl.BlockSpec((rows, HDIM), lambda h: (0, head0 + h))
    edge = pl.BlockSpec((REACH, HDIM), lambda h: (0, h))
    line = pl.BlockSpec((1, 1, WRAP), lambda h: (head0 + h, 0, 0))
    width = heads * HDIM
    sds = jax.ShapeDtypeStruct
    flops = 12 * heads * rows * BAND * HDIM
    return pl.pallas_call(
        attention_kernel,
        grid=(heads,),
        in_specs=[pl.BlockSpec(memory_space=pltpu.SMEM), line, shifted, shifted, shifted, shifted,
                  pl.BlockSpec((REACH, HDIM), lambda h: (0, h)), pl.BlockSpec((REACH, HDIM), lambda h: (0, h))],
        out_specs=[whole, whole, whole, edge, edge, edge, edge,
                   pl.BlockSpec((1, 1, WRAP), lambda h: (h, 0, 0))],
        out_shape=[
            sds((rows, width), jnp.bfloat16), sds((rows, width), jnp.bfloat16), sds((rows, width), jnp.bfloat16),
            sds((REACH, width), jnp.bfloat16), sds((REACH, width), jnp.bfloat16),
            sds((REACH, width), jnp.float32), sds((REACH, width), jnp.float32),
            sds((heads, 1, WRAP), jnp.float32),
        ],
        scratch_shapes=[
            pltpu.VMEM((rows + REACH, HDIM), jnp.bfloat16), pltpu.VMEM((rows + REACH, HDIM), jnp.bfloat16),
            pltpu.VMEM((rows + REACH, HDIM), jnp.float32), pltpu.VMEM((rows + REACH, HDIM), jnp.float32),
            pltpu.VMEM((TILE, WRAP), jnp.float32),
        ],
        cost_estimate=pl.CostEstimate(flops=flops * 2, bytes_accessed=heads * rows * HDIM * 20, transcendentals=heads * rows * BAND),
    )(first, bias_rows, query, keys, values, upstream, halo_k, halo_v)


def swap(block, bit):
    size = lax.axis_size("sp")
    return lax.ppermute(block, "sp", [(i, i ^ (1 << bit)) for i in range(size)])


def side(pieces, lead, want):
    low = len(pieces)
    return [pieces[r] for r in range(low) if (r >> lead & 1) == want]


def product(lhs, grads):
    parts = [jnp.einsum("td,tc->dc", piece, grads, preferred_element_type=jnp.float32) for piece in lhs]
    return parts


def leading(pieces, grads, order):
    return jnp.concatenate([p.astype(jnp.bfloat16) for p in product(side(pieces, order[0], 1), grads)], axis=0)


def remainder(pieces, grads, order, came):
    total = jnp.concatenate(product(side(pieces, order[0], 0), grads), axis=0)
    return total + came.astype(jnp.float32)


def split(total, kept, bit):
    depth = total.shape[0] // len(kept)
    out = [i for i, r in enumerate(kept) if r >> bit & 1]
    stay = [i for i, r in enumerate(kept) if not r >> bit & 1]
    pick = lambda which: jnp.concatenate([total[i * depth : (i + 1) * depth] for i in which], axis=0)
    return pick(out).astype(jnp.bfloat16), pick(stay), [kept[i] for i in stay]


def staged_local(inputs, w_query, w_key, w_value, rel_table, out_grad):
    rows, model = inputs.shape
    head_count = w_query.shape[1] // HDIM
    size = lax.axis_size("sp")
    bits = size.bit_length() - 1
    me = lax.axis_index("sp")
    first = me.reshape(1)
    far = rel_table[:, 2 * MAXREL :]
    pad = jnp.broadcast_to(far, (head_count, MAXREL))
    bias_rows = jnp.concatenate([pad, rel_table[:, :0:-1], pad], axis=1)[:, None, :]
    keys = project(inputs, w_key)
    values = project(inputs, w_value)
    halo = from_behind(jnp.concatenate([keys[rows - REACH :], values[rows - REACH :]], axis=1), "sp", 1)
    query = project(inputs, w_query)
    width = head_count * HDIM
    heads = head_count // GROUPS
    span = heads * HDIM
    depth = model // size
    block = lambda r: lax.dynamic_slice(inputs, (0, (me ^ r) * depth), (rows, depth))
    low = min(size, 4)
    members = [[r for r in range(size) if r % low == p] for p in range(low)]
    pieces = [jnp.concatenate([block(r) for r in rs], axis=1) for rs in members]
    orders, ready = chunk_plan(bits)
    grads, chunks, flying, diags = [], [], [], []
    for group in range(GROUPS):
        at = group * span
        dq, dk, dv, hdk, hdv, tk, tv, diag = attention(
            first, bias_rows, query, keys, values, out_grad,
            halo[:, at : at + span], halo[:, width + at : width + at + span], group * heads, heads)
        back = jnp.concatenate([hdk, hdv], axis=1)
        sent = leading(pieces, dq, orders[3 * group])
        if group + 1 < GROUPS:
            back, sent, query = lax.optimization_barrier((back, sent, query))
        back = from_behind(back, "sp", -1).astype(jnp.float32)
        flying.append(swap(sent, orders[3 * group][0]))
        dk = lax.dynamic_update_slice(dk, (tk + back[:, :span]).astype(jnp.bfloat16), (rows - REACH, 0))
        dv = lax.dynamic_update_slice(dv, (tv + back[:, span:]).astype(jnp.bfloat16), (rows - REACH, 0))
        for i, grad in ((1, dk), (2, dv)):
            order = orders[3 * group + i]
            sent = leading(pieces, grad, order)
            flying.append(swap(sent, order[0]))
        grads.append((dq, dk, dv))
        chunks.extend((dq, dk, dv))
        diags.append(diag)
    count = len(chunks)
    kept = [[r for p in range(low) if not p >> order[0] & 1 for r in members[p]] for order in orders]
    held = [None] * count
    steps = sorted(((c, s) for c in range(count) for s in range(bits)), key=lambda cs: (ready[cs[0]] + 0.95 * cs[1], cs))
    last, done, hop = None, 0, 0
    diag = jnp.concatenate(diags, axis=0)[:, 0, :]
    table_came = swap(diag, 0)
    for c, stage in steps:
        came = flying[c]
        if last is not None:
            came, held[last] = lax.optimization_barrier((came, held[last]))
        if stage == 0:
            held[c] = remainder(pieces, chunks[c], orders[c], came)
        else:
            held[c] = held[c] + came.astype(jnp.float32)
        if stage + 1 < bits:
            bit = orders[c][stage + 1]
            out, held[c], kept[c] = split(held[c], kept[c], bit)
            flying[c] = swap(out, bit)
        last = c
        done += 1
        if hop < bits and done >= len(steps) * (hop + 1) // (bits + 1):
            came, held[c] = lax.optimization_barrier((table_came, held[c]))
            diag = diag + came
            hop += 1
            if hop < bits:
                table_came = swap(diag, hop)
    sums = [held[3 * group : 3 * group + 3] for group in range(GROUPS)]
    query_grad, key_grad, value_grad = [jnp.concatenate(parts, axis=1) for parts in zip(*grads)]
    wq, wk, wv = [jnp.concatenate(parts, axis=1) for parts in zip(*sums)]
    top = jnp.sum(diag[:, : MAXREL + 1], axis=1, keepdims=True) + jnp.sum(diag[:, 3 * MAXREL :], axis=1, keepdims=True)
    table_grad = jnp.concatenate(
        [jnp.zeros((head_count, 1), jnp.float32), diag[:, MAXREL + 1 : 3 * MAXREL][:, ::-1], top], axis=1)
    return query_grad, key_grad, value_grad, wq, wk, wv, table_grad


def fused_kernel(
    ways, table_ref, x_hbm, wq_hbm, wk_hbm, wv_hbm, g_hbm,
    dqb, dkb, dvb, final, diag_ref,
    bias_ref, xb, wb, gb, qb, kv, dk_acc, dv_acc, band_acc, grads_t,
    near_out, near_in, own, far_out, far_in, relay_in, early_out, early_in, early_relay_in, early_all, early_hold, early_own, late_out, late_in,
    back_out, back_in, diag_mine, diag_in,
    load_sem, halo_s, halo_r, back_s, back_r, near_s, near_r, far_s, far_r, relay_r,
    early_s, early_r, early_relay_r, late_s, late_r, diag_s, diag_r,
):
    across, along, early = ways
    size = across * along
    heads, rows, _ = qb.shape
    model = xb.shape[1]
    depth = model // size
    scale = HDIM ** (-0.5)
    me = lax.axis_index("sp")
    xi = lax.rem(me, across)
    zi = me // across

    tail = pl.ds(rows - REACH, REACH)
    head_rows = pl.ds(0, rows - REACH)
    loads = []

    def load(src, dst):
        loads.append(pltpu.make_async_copy(src, dst, load_sem.at[len(loads)]))
        return loads[-1]

    def load_rows(at):
        span = lambda b: pl.ds(b * depth, depth)
        return [load(x_hbm.at[at, span(z * across + x)], xb.at[at, span(x * along + z)])
                for x in range(across) for z in range(along)]

    def load_weight(src, which):
        return [load(src.at[:, x], wb.at[which, x]) for x in range(across)]

    tail_ready = load_rows(tail)
    weight_ready = [load_weight(wk_hbm, 0), load_weight(wv_hbm, 1)]
    rest_ready = load_rows(head_rows) + load_weight(wq_hbm, 2)
    grad_ready = [load(g_hbm.at[:, pl.ds(h * HDIM, HDIM)], gb.at[h]) for h in range(heads)]
    for copy in loads:
        copy.start()

    barrier = pltpu.get_barrier_semaphore()
    for k in range(1, size):
        pl.semaphore_signal(barrier, 1, device_id={"sp": lax.rem(me + k, size)})

    def halo(h):
        return pltpu.make_async_remote_copy(
            kv.at[:, h, pl.ds(rows, REACH)], kv.at[:, h, pl.ds(0, REACH)],
            halo_s.at[h], halo_r.at[h], device_id={"sp": lax.rem(me + 1, size)})

    def back(h):
        return pltpu.make_async_remote_copy(
            back_out.at[h], back_in.at[h], back_s.at[h], back_r.at[h],
            device_id={"sp": lax.rem(me + size - 1, size)})

    def used(h):
        return pl.ds(HDIM, 2 * HDIM) if h < early else pl.ds(0, 3 * HDIM)

    def at_z(z):
        return {"sp": z * across + xi}

    def at_x(x):
        return {"sp": zi * across + x}

    def near(h, dx, z):
        return pltpu.make_async_remote_copy(
            near_out.at[h, dx - 1, z, used(h)], near_in.at[h, dx - 1, z, used(h)],
            near_s.at[h, dx - 1, z], near_r.at[h, dx - 1, z], device_id=at_x(lax.rem(xi + dx, across)))

    def far(h, z):
        slot = lax.rem(z - zi + along, along) - 1
        return pltpu.make_async_remote_copy(
            far_out.at[h, z, used(h)], far_in.at[h, slot, used(h)], far_s.at[h, z], far_r.at[h, slot],
            device_id=at_z(z))

    def relay(h, z):
        step = jnp.where(z > zi, 1, -1)
        return pltpu.make_async_remote_copy(
            far_out.at[h, z, used(h)], relay_in.at[h, used(h)], far_s.at[h, z], relay_r.at[h],
            device_id=at_z(lax.rem(zi + step + along, along)))

    def early_copy(u, z):
        slot = lax.rem(z - zi + along, along) - 1
        return pltpu.make_async_remote_copy(
            early_out.at[u, z], early_in.at[u, slot], early_s.at[u, z], early_r.at[u, slot], device_id=at_z(z))

    def early_relay(u, z):
        step = jnp.where(z > zi, 1, -1)
        return pltpu.make_async_remote_copy(
            early_out.at[u, z], early_relay_in.at[u], early_s.at[u, z], early_relay_r.at[u],
            device_id=at_z(lax.rem(zi + step + along, along)))

    def late_copy(u, dx):
        return pltpu.make_async_remote_copy(
            late_out.at[u, dx - 1], late_in.at[u, dx - 1], late_s.at[u, dx - 1], late_r.at[u, dx - 1],
            device_id=at_x(lax.rem(xi + dx, across)))

    relayed = along > 3

    def order(step):
        place = 0
        for z in range(along):
            others = sorted((t for t in range(along) if t != z), key=lambda t: hop_rank(z, t, along)) + [z]
            place = place + jnp.where(zi == z, others[step], 0)
        return place

    def share(k):
        return pltpu.make_async_remote_copy(
            diag_mine, diag_in.at[k - 1], diag_s.at[k - 1], diag_r.at[k - 1],
            device_id={"sp": lax.rem(me + k, size)})

    def project_rows(at, which, first, count):
        cols = pl.ds(first * HDIM, count * HDIM)
        weight = wb[which, :, :, :, cols].reshape(model, count * HDIM)
        value = jnp.dot(xb[at], weight, preferred_element_type=jnp.float32).astype(jnp.bfloat16)
        return [(first + h, value[:, h * HDIM : (h + 1) * HDIM]) for h in range(count)]

    @pl.when(me == 0)
    def _():
        kv[:, :, :REACH] = jnp.zeros((2, heads, REACH, HDIM), jnp.bfloat16)

    @pl.when(me == size - 1)
    def _():
        back_in[...] = jnp.zeros_like(back_in)

    entries = table_ref.shape[1]
    entry = lax.broadcasted_iota(jnp.int32, (entries, WRAP), 0)
    spot = lax.broadcasted_iota(jnp.int32, (entries, WRAP), 1)
    near_diag = (spot >= MAXREL) & (spot < 3 * MAXREL)
    pick = jnp.where(entry == jnp.where(near_diag, 3 * MAXREL - spot, 2 * MAXREL), 1.0, 0.0)
    lines = jnp.dot(table_ref[...], pick, precision=lax.Precision.HIGHEST, preferred_element_type=jnp.float32)
    for h in range(heads):
        bias_ref[h] = lines[h : h + 1]

    for copy in tail_ready:
        copy.wait()
    for which in range(2):
        for copy in weight_ready[which]:
            copy.wait()
        for h, value in project_rows(tail, which, 0, heads):
            kv[which, h, pl.ds(rows, REACH)] = value
    pl.semaphore_wait(barrier, size - 1)

    @pl.when(me < size - 1)
    def _():
        for h in range(heads):
            halo(h).start()

    def project(first, count):
        def chunk(c, carry):
            lo = pl.multiple_of(c * REACH, REACH)
            at = pl.ds(lo, REACH)
            for which in range(2):
                for h, value in project_rows(at, which, first, count):
                    kv[which, h, pl.ds(pl.multiple_of(lo + REACH, REACH), REACH)] = value
            for h, value in project_rows(at, 2, first, count):
                qb[h, at] = value
            return carry

        lax.fori_loop(0, rows // REACH - 1, chunk, 0)
        for h, value in project_rows(tail, 2, first, count):
            qb[h, tail] = value

    for copy in rest_ready:
        copy.wait()
    lead_heads = max(heads // 2, 1)
    project(0, lead_heads)
    for copy in grad_ready:
        copy.wait()

    row = lax.broadcasted_iota(jnp.int32, (TILE, BAND), 0)
    col = lax.broadcasted_iota(jnp.int32, (TILE, BAND), 1)
    start = row // SEG * SEG
    seen = (col >= start) & (col < start + REACH + SEG)
    is_first = me == 0

    def run_blocks(h, first, count, bias):
        spans = [(blk * TILE, blk * TILE + TILE, blk * TILE + BAND) for blk in range(first, first + count)]
        q = [qb[h, lo:hi] for lo, hi, end in spans]
        g = [gb[h, lo:hi] for lo, hi, end in spans]
        k = [kv[0, h, lo:end] for lo, hi, end in spans]
        v = [kv[1, h, lo:end] for lo, hi, end in spans]
        each = range(count)
        s = [contract(q[i], k[i], ((1,), (1,))) * scale + bias for i in each]
        dp = [contract(g[i], v[i], ((1,), (1,))) for i in each]
        s = [
            jnp.where(is_first & (col < REACH - lo), -jnp.inf, x) if lo < REACH else x
            for x, (lo, hi, end) in zip(s, spans)
        ]
        m = [jnp.max(x, axis=1, keepdims=True) for x in s]
        e = [jnp.exp(s[i] - m[i]) for i in each]
        p = [x * (1.0 / jnp.sum(x, axis=1, keepdims=True)) for x in e]
        p_low = [x.astype(jnp.bfloat16) for x in p]
        out = [contract(p_low[i], v[i], ((1,), (0,))).astype(jnp.bfloat16) for i in each]
        out_dot = [
            jnp.sum(g[i].astype(jnp.float32) * out[i].astype(jnp.float32), axis=1, keepdims=True) for i in each
        ]
        ds = [p[i] * (dp[i] - out_dot[i]) for i in each]
        ds_low = [x.astype(jnp.bfloat16) for x in ds]
        band_acc[h, :, :BAND] += functools.reduce(lambda a, b: a + b, ds)
        dq = [(contract(ds_low[i], k[i], ((1,), (0,))) * scale).astype(jnp.bfloat16) for i in each]
        dk = [contract(ds_low[i], q[i], ((0,), (0,))) for i in each]
        dv = [contract(p_low[i], g[i], ((0,), (0,))) for i in each]
        for i, (lo, hi, end) in enumerate(spans):
            dqb[h, lo:hi] = dq[i]
            grads_t[h, :HDIM, lo:hi] = dq[i].T
            dk_acc[h, lo:end] += dk[i]
            dv_acc[h, lo:end] += dv[i]

    together = REACH // TILE

    def bias_of(h):
        wide = jnp.broadcast_to(bias_ref[h], (TILE, WRAP))
        bias = pltpu.roll(wide, 0, 1, stride=1, stride_axis=0)[:, :BAND]
        return jnp.where(seen, bias, -jnp.inf)

    def attend_edge(h):
        dk_acc[h] = jnp.zeros(dk_acc.shape[1:], jnp.float32)
        dv_acc[h] = jnp.zeros(dv_acc.shape[1:], jnp.float32)
        band_acc[h] = jnp.zeros(band_acc.shape[1:], jnp.float32)
        bias = bias_of(h)

        @pl.when(me > 0)
        def _():
            halo(h).wait_recv()

        run_blocks(h, 0, REACH // TILE, bias)
        back_out[h, 0] = (dk_acc[h, :REACH] * scale).astype(jnp.bfloat16)
        back_out[h, 1] = dv_acc[h, :REACH].astype(jnp.bfloat16)

        @pl.when(me > 0)
        def _():
            back(h).start()

    def attend(h):
        bias = bias_of(h)
        for blk in range(REACH // TILE, rows // TILE, together):
            run_blocks(h, blk, together, bias)
        total = band_acc[h]
        half = TILE // 2
        while half >= 1:
            total = total[:half] + pltpu.roll(total[half:], WRAP - half, 1)
            half //= 2
        diag_mine[h] = total

        @pl.when(me < size - 1)
        def _():
            back(h).wait_recv()

        dk_acc[h, rows:] += back_in[h, 0].astype(jnp.float32) * (1.0 / scale)
        dv_acc[h, rows:] += back_in[h, 1].astype(jnp.float32)
        for lo in range(0, rows, REACH):
            dk = (dk_acc[h, REACH + lo : 2 * REACH + lo] * scale).astype(jnp.bfloat16)
            dv = dv_acc[h, REACH + lo : 2 * REACH + lo].astype(jnp.bfloat16)
            dkb[h, lo : lo + REACH] = dk
            dvb[h, lo : lo + REACH] = dv
            grads_t[h, HDIM : 2 * HDIM, lo : lo + REACH] = dk.T
            grads_t[h, 2 * HDIM :, lo : lo + REACH] = dv.T

    def product(h, part, x):
        cols = pl.ds(pl.multiple_of(x * along * depth, along * depth), along * depth)
        value = jnp.dot(grads_t[h, part], xb[:, cols], preferred_element_type=jnp.float32)
        return [value[:, z * depth : (z + 1) * depth] for z in range(along)]

    def ends(z):
        return ((zi == 0) & (z == along - 1)) | ((zi == along - 1) & (z == 0))

    def joins(z):
        return ((zi == 1) & (z == along - 1)) | ((zi == along - 2) & (z == 0))

    def arrives(dz):
        if not relayed:
            return None
        source = lax.rem(zi - dz + along, along)
        return jnp.logical_not(((source == 0) & (zi == along - 1)) | ((source == along - 1) & (zi == 0)))

    def multiply_early(h):
        for x in range(across):
            for z, value in enumerate(product(h, pl.ds(0, HDIM), x)):
                early_all[z, :, x * depth : (x + 1) * depth] = value
        for step in range(along):
            z = order(step)
            value = early_all[z]
            if step == along - 1:
                early_own[h] = value
            elif relayed:
                @pl.when(joins(z))
                def _():
                    early_hold[h] = value

                @pl.when(jnp.logical_not(joins(z)))
                def _():
                    early_out[h, z] = value.astype(jnp.bfloat16)

                @pl.when(ends(z))
                def _():
                    early_relay(h, z).start()

                @pl.when(jnp.logical_not(ends(z) | joins(z)))
                def _():
                    early_copy(h, z).start()
            else:
                early_out[h, z] = value.astype(jnp.bfloat16)
                early_copy(h, z).start()

    def join_early(u):
        if not relayed:
            return
        z = order(along - 2)

        @pl.when(joins(z))
        def _():
            early_relay(u, z).wait_recv()
            early_out[u, z] = (early_hold[u] + early_relay_in[u].astype(jnp.float32)).astype(jnp.bfloat16)
            early_copy(u, z).start()

    def multiply(h):
        for dx in range(1, across):
            for z, value in enumerate(product(h, used(h), lax.rem(xi + dx, across))):
                near_out[h, dx - 1, z, used(h)] = value.astype(jnp.bfloat16)
            for step in range(along - 1):
                near(h, dx, order(step)).start()
        for z, value in enumerate(product(h, used(h), xi)):
            own[h, z, used(h)] = value

    def send_own(h):
        for dx in range(1, across):
            near(h, dx, zi).start()

    def collect(h, z):
        total = own[h, z, used(h)]
        for dx in range(1, across):
            near(h, dx, z).wait_recv()
            total = total + near_in[h, dx - 1, z, used(h)].astype(jnp.float32)
        return total

    def forward(h):
        for step in range(along - 1):
            z = order(step)
            total = collect(h, z)
            if not relayed:
                far_out[h, z, used(h)] = total.astype(jnp.bfloat16)
                far(h, z).start()
                continue

            @pl.when(joins(z))
            def _():
                relay(h, z).wait_recv()
                far_out[h, z, used(h)] = (total + relay_in[h, used(h)].astype(jnp.float32)).astype(jnp.bfloat16)

            @pl.when(jnp.logical_not(joins(z)))
            def _():
                far_out[h, z, used(h)] = total.astype(jnp.bfloat16)

            @pl.when(ends(z))
            def _():
                relay(h, z).start()

            @pl.when(jnp.logical_not(ends(z)))
            def _():
                far(h, z).start()

    def turn(u):
        for dz in range(1, along):
            def add():
                early_copy(u, lax.rem(zi + dz, along)).wait_recv()
                early_own[u] += early_in[u, dz - 1].astype(jnp.float32)

            if relayed:
                pl.when(arrives(dz))(add)
            else:
                add()
        for dx in range(1, across):
            cols = pl.ds(pl.multiple_of(lax.rem(xi + dx, across) * depth, depth), depth)
            late_out[u, dx - 1] = early_own[u, :, cols].astype(jnp.bfloat16)
            late_copy(u, dx).start()

    def deliver(h, i, total):
        final[i, :, h * HDIM : (h + 1) * HDIM] = total.T

    def finish_early(u):
        total = early_own[u, :, pl.ds(pl.multiple_of(xi * depth, depth), depth)]
        for dx in range(1, across):
            late_copy(u, dx).wait_recv()
            total = total + late_in[u, dx - 1].astype(jnp.float32)
        deliver(u, 0, total)

    def finish(h):
        lead = 1 if h < early else 0
        own[h, zi, used(h)] = collect(h, zi)
        for dz in range(1, along):
            def add():
                far(h, lax.rem(zi + dz, along)).wait_recv()
                own[h, zi, used(h)] += far_in[h, dz - 1, used(h)].astype(jnp.float32)

            if relayed:
                pl.when(arrives(dz))(add)
            else:
                add()
        for i in range(lead, 3):
            deliver(h, i, own[h, zi, i * HDIM : (i + 1) * HDIM])

    for h in range(heads):
        if h == 0:
            attend_edge(0)
        if h == 1:
            for other in range(1, lead_heads):
                attend_edge(other)
            if lead_heads < heads:
                project(lead_heads, heads - lead_heads)
            join_early(0)
            for other in range(lead_heads, heads):
                attend_edge(other)
            forward(0)
            send_own(0)
        attend(h)
        if h < early:
            multiply_early(h)
        multiply(h)
        if 0 < h < early:
            join_early(h)
        if h > 1:
            forward(h - 1)
        if 2 <= h < early + 2:
            turn(h - 2)
    for k in range(1, size):
        share(k).start()
    for u in range(max(heads - 2, 0), early):
        turn(u)
    for h in range(1, heads):
        send_own(h)
    if heads > 1:
        forward(heads - 1)
    for h in range(heads):
        finish(h)
    for u in range(early):
        finish_early(u)
    total = diag_mine[...]
    for k in range(1, size):
        share(k).wait_recv()
        total = total + diag_in[k - 1]
    diag_ref[...] = total
    for k in range(1, size):
        share(k).wait_send()

    @pl.when(me < size - 1)
    def _():
        for h in range(heads):
            halo(h).wait_send()

    @pl.when(me > 0)
    def _():
        for h in range(heads):
            back(h).wait_send()

    for h in range(heads):
        for step in range(along - 1):
            far(h, order(step)).wait_send()
        for dx in range(1, across):
            for z in range(along):
                near(h, dx, z).wait_send()
    for u in range(early):
        for step in range(along - 1):
            early_copy(u, order(step)).wait_send()
        for dx in range(1, across):
            late_copy(u, dx).wait_send()


def hop_rank(here, there, along):
    far_end = abs(there - here) == along - 1
    joined = (here == 1 and there == along - 1) or (here == along - 2 and there == 0)
    return (joined, not far_end, -abs(there - here), there)


def fused_local(inputs, w_query, w_key, w_value, rel_table, out_grad):
    rows, model = inputs.shape
    width = w_query.shape[1]
    heads = width // HDIM
    size = lax.axis_size("sp")
    across, along = grid_of(size)
    early = heads // 2
    depth = model // size
    sds = jax.ShapeDtypeStruct
    bf16, f32 = jnp.bfloat16, jnp.float32
    any_space = pl.BlockSpec(memory_space=pl.ANY)
    vmem = pl.BlockSpec(memory_space=pltpu.VMEM)
    dma = pltpu.SemaphoreType.DMA
    *blocks, diag = pl.pallas_call(
        functools.partial(fused_kernel, (across, along, early)),
        in_specs=[vmem] + [any_space] * 5,
        out_specs=[vmem] * 5,
        out_shape=[pltpu.VMEM((heads, rows, HDIM), bf16)] * 3 + [
            pltpu.VMEM((3, depth, width), f32), pltpu.VMEM((heads, 1, WRAP), f32)],
        scratch_shapes=[
            pltpu.VMEM((heads, 1, WRAP), f32),
            pltpu.VMEM((rows, model), bf16),
            pltpu.VMEM((3, across, along, depth, width), bf16),
            pltpu.VMEM((heads, rows, HDIM), bf16),
            pltpu.VMEM((heads, rows, HDIM), bf16),
            pltpu.VMEM((2, heads, rows + REACH, HDIM), bf16),
            pltpu.VMEM((heads, rows + REACH, HDIM), f32),
            pltpu.VMEM((heads, rows + REACH, HDIM), f32),
            pltpu.VMEM((heads, TILE, WRAP), f32),
            pltpu.VMEM((heads, 3 * HDIM, rows), bf16),
            pltpu.VMEM((heads, across - 1, along, 3 * HDIM, depth), bf16),
            pltpu.VMEM((heads, across - 1, along, 3 * HDIM, depth), bf16),
            pltpu.VMEM((heads, along, 3 * HDIM, depth), f32),
            pltpu.VMEM((heads, along, 3 * HDIM, depth), bf16),
            pltpu.VMEM((heads, along - 1, 3 * HDIM, depth), bf16),
            pltpu.VMEM((heads, 3 * HDIM, depth), bf16),
            pltpu.VMEM((early, along, HDIM, across * depth), bf16),
            pltpu.VMEM((early, along - 1, HDIM, across * depth), bf16),
            pltpu.VMEM((early, HDIM, across * depth), bf16),
            pltpu.VMEM((along, HDIM, across * depth), f32),
            pltpu.VMEM((early, HDIM, across * depth), f32),
            pltpu.VMEM((early, HDIM, across * depth), f32),
            pltpu.VMEM((early, across - 1, HDIM, depth), bf16),
            pltpu.VMEM((early, across - 1, HDIM, depth), bf16),
            pltpu.VMEM((heads, 2, REACH, HDIM), bf16),
            pltpu.VMEM((heads, 2, REACH, HDIM), bf16),
            pltpu.VMEM((heads, 1, WRAP), f32),
            pltpu.VMEM((size - 1, heads, 1, WRAP), f32),
            dma((2 * size + 3 * across + heads,)),
            dma((heads,)), dma((heads,)), dma((heads,)), dma((heads,)),
            dma((heads, across - 1, along)), dma((heads, across - 1, along)),
            dma((heads, along)), dma((heads, along - 1)), dma((heads,)),
            dma((early, along)), dma((early, along - 1)), dma((early,)), dma((early, across - 1)), dma((early, across - 1)),
            dma((size - 1,)), dma((size - 1,)),
        ],
        compiler_params=pltpu.CompilerParams(collective_id=0, has_side_effects=True, vmem_limit_bytes=52 * 2**20),
    )(rel_table, inputs, *(w.reshape(along, across, depth, width) for w in (w_query, w_key, w_value)), out_grad)
    return pl.pallas_call(
        publish,
        in_specs=[vmem] * 5,
        out_specs=[any_space] * 6 + [vmem],
        out_shape=[sds((rows, width), bf16)] * 3 + [sds((depth, width), f32)] * 3 + [sds(rel_table.shape, f32)],
        scratch_shapes=[dma((3, heads)), dma((3,))],
        compiler_params=pltpu.CompilerParams(vmem_limit_bytes=8 * 2**20),
    )(*blocks, diag)


def publish(dqb, dkb, dvb, final, diag, dq, dk, dv, gq, gk, gv, table, sem, final_sem):
    copies = [pltpu.make_async_copy(final.at[i], out, final_sem.at[i]) for i, out in enumerate((gq, gk, gv))]
    for i, (buf, out) in enumerate(((dqb, dq), (dkb, dk), (dvb, dv))):
        for h in range(buf.shape[0]):
            copies.append(pltpu.make_async_copy(buf.at[h], out.at[:, h * HDIM : (h + 1) * HDIM], sem.at[i, h]))
    for copy in copies:
        copy.start()
    heads, entries = table.shape
    spot = lax.broadcasted_iota(jnp.int32, (WRAP, entries), 0)
    entry = lax.broadcasted_iota(jnp.int32, (WRAP, entries), 1)
    inner = (spot + entry == 3 * MAXREL) & (entry > 0) & (entry < 2 * MAXREL)
    outer = (entry == 2 * MAXREL) & ((spot <= MAXREL) | (spot >= 3 * MAXREL))
    pick = jnp.where(inner | outer, 1.0, 0.0)
    lines = diag[...].reshape(heads, WRAP)
    table[...] = jnp.dot(lines, pick, precision=lax.Precision.HIGHEST, preferred_element_type=jnp.float32)
    for copy in copies:
        copy.wait()


def grid_of(size):
    across = 1 << ((size.bit_length() - 1) // 2)
    return across, size // across


def fits(size, rows, model, width):
    across, along = grid_of(size)
    depth = model // size
    held = 2 * (rows * model + 3 * model * width + 7 * rows * width + 3 * model * width * 2) + 6 * model * width * 2
    return across > 1 and along > 2 and width >= 4 * HDIM and depth % HDIM == 0 and rows % REACH == 0 and rows > REACH and held < 56 * 2**20


def local(*args):
    inputs, w_query = args[:2]
    if fits(lax.axis_size("sp"), *inputs.shape, w_query.shape[1]):
        return fused_local(*args)
    return staged_local(*args)


def chunk_plan(bits):
    plain = list(range(bits))
    turned = [1, 0] + plain[2:] if bits > 1 else plain
    count = 3 * GROUPS
    orders = [plain] * (count - 2) + [turned] * 2
    ready = [1.0, 3.0, 4.0, 2.0, 3.9, 4.1]
    return orders, ready


def solution(mesh):
    placed = (
        P("sp", None),
        P(None, "tp"),
        P(None, "tp"),
        P(None, "tp"),
        P("tp", None),
        P("sp", "tp"),
    )
    return jax.shard_map(
        local,
        mesh=mesh,
        in_specs=placed,
        out_specs=(
            P("sp", "tp"),
            P("sp", "tp"),
            P("sp", "tp"),
            P("sp", "tp"),
            P("sp", "tp"),
            P("sp", "tp"),
            P("tp", None),
        ),
        check_vma=False,
    )
```
